32 devices in a mesh: sp: 16 (over z, y, x), tp: 2 (over core).
Axes of the slice: x: 2, y: 2, z: 4, core: 2. Of those that a mesh axis runs over, the one named last changes fastest.
Arguments:
- residual: bfloat16 [4096, 2048], P(('sp', 'tp')), may hold values from -6 to 6
- pool_input: bfloat16 [4096, 1024], P('sp', 'tp'), may hold values from -6 to 6
- group_maps: bfloat16 [8, 128, 128], replicated, may hold values from -0.5 to 0.5
- pool_scale: float32 [1024], replicated, may hold values from 0.1 to 1.9
- out_proj: bfloat16 [1024, 2048], replicated, may hold values from -0.1875 to 0.1875
- norm_gain: float32 [2048], replicated, may hold values from 0.1 to 1.9
- shared_gate: bfloat16 [2048, 512], replicated, may hold values from -0.125 to 0.125
- shared_up: bfloat16 [2048, 512], replicated, may hold values from -0.125 to 0.125
- shared_down: bfloat16 [512, 2048], replicated, may hold values from -0.25 to 0.25
- expert_gate: bfloat16 [32, 2048, 512], P(('sp', 'tp')), may hold values from -0.125 to 0.125
- expert_up: bfloat16 [32, 2048, 512], P(('sp', 'tp')), may hold values from -0.125 to 0.125
- expert_down: bfloat16 [32, 512, 2048], P(('sp', 'tp')), may hold values from -0.25 to 0.25
- expert_ids: int32 [4096, 4], P(('sp', 'tp')), may hold values from 0 to 31, all different within a row; in each aligned block of 128 rows (0 to 127, 128 to 255, ...) at most 24 rows name the same one
- route_score: float32 [4096, 4], P(('sp', 'tp')), may hold values from 0.05 to 1
Outputs:
- output: bfloat16 [4096, 2048], P(('sp', 'tp'))
The draws below stay inside these ranges and needn't reach their ends.
Inputs may be any that keep to these rules, and one draw needn't show every extreme that they name: `expert_ids`: each row names 4 different experts; among the 128 rows of one device no expert is named more than 24 times, and in some devices' rows one expert is named exactly 24 times.
All inputs are finite; a program needn't handle non-finite values.
Results may differ from the reference program's by a relative error of at most 0.015.
Values may be sent and summed in bfloat16 or wider, within the bound.
A program may use at most 128 MiB of HBM per device.

```python
import math
import jax
import jax.numpy as jnp
import numpy as np
from jax import lax

D = 2048
POOL_GROUPS = 8
GROUP_WIDTH = 128
EXPERT_HIDDEN = 512
SHARED_HIDDEN = 512
TOPK = 4
TOK_DEV = 128
TOKENS = 4096
POOL = 1024
EXPERTS = 32
CAP = 24


def shard_levels(own_key, shape, shards, least, high):
    def one(position, parts):
        draws = jax.random.uniform(jax.random.fold_in(jax.random.fold_in(own_key, 6), position), (parts,), jnp.float32, least / len(shards), high / len(shards))
        return jnp.repeat(jnp.exp(draws), shape[position] // parts).reshape((-1,) + (1,) * (len(shape) - position - 1))

    gain = one(*shards[0])
    for cut in shards[1:]:
        gain = gain * one(*cut)
    return gain


def shared_out(stream_key, own, number, rows, amount, top, reach, lean):
    ranking = jax.random.permutation(stream_key, amount)
    heavy_load, common = portions_of(amount, rows * top, reach, lean, True), portions_of(amount, rows * top, reach, lean, False)
    places = jnp.arange(amount)

    def named(tallies, rotation):
        used = int((tallies > 0).sum())
        fixed = max(1, used // 4)
        moved = fixed + (places - fixed + rotation * (used - fixed)) % max(1, amount - fixed)
        return jnp.zeros((amount,), jnp.int32).at[ranking[jnp.where(places < fixed, places, moved)]].set(jnp.asarray(tallies, jnp.int32))

    tallies = jnp.where(number % 4 == 0, named(heavy_load, number // 4), named(common, number - number // 4 - 1))
    mixed = jax.random.permutation(jax.random.fold_in(own, 3), amount)
    source_of, taker = mixed[0:amount // 2 * 2:2], mixed[1:amount // 2 * 2:2]
    slack = jnp.minimum(tallies[source_of] - 1, reach - tallies[taker]) // 2
    slack = jnp.where((source_of == ranking[0]) | (taker == ranking[0]) | (tallies[taker] == 0), 0, jnp.maximum(slack, 0))
    moved = jax.random.randint(jax.random.fold_in(own, 4), (amount // 2,), 0, 1 << 20) % (slack + 1)
    tallies = tallies.at[source_of].add(-moved).at[taker].add(moved)
    items = jnp.searchsorted(jnp.cumsum(tallies), jnp.arange(rows * top), side="right").astype(jnp.int32)
    table = items.reshape(top, rows).T
    table = table[jax.random.permutation(jax.random.fold_in(own, 1), rows)]
    rotation = jax.random.randint(jax.random.fold_in(own, 2), (rows, 1), 0, top)
    return jnp.take_along_axis(table, (jnp.arange(top)[None, :] + rotation) % top, axis=1)


def portions_of(count, total, bound, slope, full):
    loads = [(1 << 20) // math.isqrt(rank ** slope) + 1 for rank in range(1, count + 1)]
    largest = bound if full else min(bound, max(-(-total // count), total * loads[0] // sum(loads)))
    least = 1 if total - largest >= count - 1 else 0
    given, rest = [largest] + [least] * (count - 1), total - largest - least * (count - 1)
    while rest > 0:
        free = [i for i in range(1, count) if given[i] < largest] or [i for i in range(1, count) if given[i] < bound]
        mass, budget = sum([loads[i] for i in free]), rest
        for i in free:
            more = min(bound - given[i], max(1, budget * loads[i] // mass), rest)
            given[i] = given[i] + more
            rest = rest - more
    return np.array(given)


def bell_draw(stream_key, shape, spread, bound, shards=(), kind=jnp.bfloat16):
    drawn = spread * jax.random.normal(stream_key, shape, jnp.float32)
    if shards:
        drawn = drawn * shard_levels(stream_key, shape, shards, -0.22, 0.18)
    return jnp.clip(drawn, -bound, bound).astype(kind)


def setup_inputs(seed: int = 0) -> dict:
    keys = jax.random.split(jax.random.key(seed), 15)
    residual = bell_draw(keys[0], (TOKENS, D), 1.0, 6.0, ((0, 32),))
    pool_input = bell_draw(keys[1], (TOKENS, POOL), 1.0, 6.0, ((0, 16), (1, 2)))
    group_maps = bell_draw(keys[2], (POOL_GROUPS, GROUP_WIDTH, GROUP_WIDTH), GROUP_WIDTH ** -0.5, 0.5)
    pool_scale = jnp.clip(1.0 + 0.18 * jax.random.normal(keys[3], (POOL,), jnp.float32), 0.1, 1.9)
    out_proj = bell_draw(keys[4], (POOL, D), POOL ** -0.5, 0.1875)
    norm_gain = jnp.clip(1.0 + 0.18 * jax.random.normal(keys[5], (D,), jnp.float32), 0.1, 1.9)
    shared_gate = bell_draw(keys[6], (D, SHARED_HIDDEN), D ** -0.5, 0.125)
    shared_up = bell_draw(keys[7], (D, SHARED_HIDDEN), D ** -0.5, 0.125)
    shared_down = bell_draw(keys[8], (SHARED_HIDDEN, D), SHARED_HIDDEN ** -0.5, 0.25)
    expert_gate = bell_draw(keys[9], (EXPERTS, D, EXPERT_HIDDEN), D ** -0.5, 0.125, ((0, 32),))
    expert_up = bell_draw(keys[10], (EXPERTS, D, EXPERT_HIDDEN), D ** -0.5, 0.125, ((0, 32),))
    expert_down = bell_draw(keys[11], (EXPERTS, EXPERT_HIDDEN, D), EXPERT_HIDDEN ** -0.5, 0.25, ((0, 32),))
    expert_ids_keys = jax.random.split(jax.random.fold_in(keys[12], 1), TOKENS // TOK_DEV)
    expert_ids_turns = jax.random.permutation(jax.random.fold_in(keys[12], 3), TOKENS // TOK_DEV)
    expert_ids = jax.vmap(lambda own, number: shared_out(jax.random.fold_in(keys[12], 2), own, number, TOK_DEV, EXPERTS, TOPK, CAP, 2))(expert_ids_keys, expert_ids_turns).reshape((TOKENS, TOPK))
    route_score = jnp.clip(0.05 + 0.95 * jax.random.uniform(keys[13], (TOKENS, TOPK), jnp.float32) ** shard_levels(keys[13], (TOKENS, TOPK), ((0, 32),), -0.2, 0.2), 0.05, 1.0)
    return dict(residual=residual, pool_input=pool_input, group_maps=group_maps, pool_scale=pool_scale, out_proj=out_proj, norm_gain=norm_gain, shared_gate=shared_gate, shared_up=shared_up, shared_down=shared_down, expert_gate=expert_gate, expert_up=expert_up, expert_down=expert_down, expert_ids=expert_ids, route_score=route_score)


windows = (2, 4, 8, 16)
epsilon = 1e-06
routed_scale = 2.5

def swiglu(row_block, w_gate, w_up, w_down):
    gate_part = jnp.dot(row_block, w_gate, preferred_element_type=jnp.float32)
    up_part = jnp.dot(row_block, w_up, preferred_element_type=jnp.float32)
    hidden = (jax.nn.silu(gate_part) * up_part).astype(jnp.bfloat16)
    return jnp.dot(hidden, w_down, preferred_element_type=jnp.float32)

def reference(residual, pool_input, group_maps, pool_scale, out_proj, norm_gain, shared_gate, shared_up, shared_down, expert_gate, expert_up, expert_down, expert_ids, route_score):
    length = pool_input.shape[0]
    groups = group_maps.shape[0]
    group_width = group_maps.shape[1]
    input_values = pool_input.astype(jnp.float32).reshape(length, groups, group_width)
    places = jnp.arange(length, dtype=jnp.int32)
    pooled = []
    for group_index in range(groups):
        window_span = windows[group_index % 4]
        group_column = input_values[:, group_index]
        padded = jnp.pad(group_column, ((window_span - 1, 0), (0, 0)))
        running_sum = padded[window_span - 1:]
        for offset_shift in range(1, window_span):
            running_sum = running_sum + padded[window_span - 1 - offset_shift:window_span - 1 - offset_shift + length]
        divisor = jnp.minimum(places + 1, window_span).astype(jnp.float32)[:, None]
        pooled.append(running_sum / divisor)
    pooled = jnp.stack(pooled, axis=1)
    contrast = (pooled - input_values).astype(jnp.bfloat16)
    mapped = jnp.einsum('sgc,gcd->sgd', contrast.astype(jnp.float32), group_maps.astype(jnp.float32))
    mixed_rows = (mapped.reshape(length, groups * group_width) * pool_scale).astype(jnp.bfloat16)
    projected = jnp.dot(mixed_rows, out_proj, preferred_element_type=jnp.float32)
    settled = (residual.astype(jnp.float32) + projected).astype(jnp.bfloat16)
    settled_wide = settled.astype(jnp.float32)
    inverse_rms = lax.rsqrt(lax.optimization_barrier(jnp.mean(settled_wide * settled_wide, axis=-1, keepdims=True)) + epsilon)
    normed = (settled_wide * inverse_rms * norm_gain).astype(jnp.bfloat16)
    shared = swiglu(normed, shared_gate, shared_up, shared_down)
    weights = route_score / lax.optimization_barrier(jnp.sum(route_score, axis=-1, keepdims=True)) * routed_scale
    experts = expert_gate.shape[0]
    top_count = expert_ids.shape[1]
    assigned = length * top_count
    flat_ids = expert_ids.reshape(assigned).astype(jnp.int32)
    sort_order = jnp.argsort(flat_ids, stable=True).astype(jnp.int32)
    sorted_ids = flat_ids[sort_order]
    counts = jnp.bincount(flat_ids, length=experts).astype(jnp.int32)
    starts = jnp.cumsum(counts).astype(jnp.int32) - counts
    expert_depth = EXPERTS * CAP
    slot_rank = jnp.arange(assigned, dtype=jnp.int32) - starts[sorted_ids]
    slot_index = sorted_ids * expert_depth + slot_rank
    slot_token = jnp.zeros((experts * expert_depth,), jnp.int32).at[slot_index].set(sort_order // top_count)
    slot_weight = jnp.zeros((experts * expert_depth,), jnp.float32).at[slot_index].set(weights.reshape(assigned)[sort_order])

    def one_expert(routed, inputs):
        token_index, slot_factor, w_gate, w_up, w_down = inputs
        expert_rows = swiglu(normed[token_index], w_gate, w_up, w_down).astype(jnp.bfloat16)
        return (routed.at[token_index].add(slot_factor[:, None] * expert_rows.astype(jnp.float32)), None)
    routed, _ = lax.scan(one_expert, jnp.zeros((length, D), jnp.float32), (slot_token.reshape(experts, expert_depth), slot_weight.reshape(experts, expert_depth), expert_gate, expert_up, expert_down))
    return (settled_wide + shared + routed).astype(jnp.bfloat16)
```

```python
import functools
import math

import jax
import jax.numpy as jnp
from jax import lax
from jax.experimental import pallas as pl
from jax.experimental.pallas import tpu as pltpu
from jax.sharding import PartitionSpec as P

windows = (2, 4, 8, 16)
epsilon = 1e-06
routed_scale = 2.5
halo_rows = 16
NOP, ARRIVE, EXPERT, COMBINE, SHARED = range(5)


def layer_count(size_sp):
    return max(d for d in range(1, math.isqrt(size_sp) + 1) if size_sp % d == 0)


END = (
    "a0", "a1", "s0", "a2", "a3", "a4", "a5", "a6", "e2",
    "a7", "c2", "e3", "e1", "c3", "c1", "e0", "c0",
)
MIDDLE = (
    "a0", "a1", "s0", "a2", "a3", "a4", "a5", "e3",
    "e2", "e1", "e0", "c2", "c3", "c0", "c1",
)


def steps_of(z, layers):
    last = layers - 1
    if layers == 4:
        kinds = {"a": ARRIVE, "e": EXPERT, "c": COMBINE, "s": SHARED}
        steps = []
        for word in END if z in (0, last) else MIDDLE:
            value = int(word[1:])
            if word[0] in "ec" and 2 * z > last:
                value = last - value
            steps.append((kinds[word[0]], value))
        return steps
    at = lambda r: [s for s in (z - r, z + r) if 0 <= s < layers]
    reach = max(z, last - z)
    steps = [(ARRIVE, 0), (ARRIVE, 1), (SHARED, 0)]
    for r in range(1, reach + 1):
        steps += [(ARRIVE, 2 * r), (ARRIVE, 2 * r + 1)]
        steps += [(EXPERT, s) for s in sorted(set(at(r - 1)))]
    steps += [(EXPERT, s) for s in at(reach)]
    for r in range(reach, 0, -1):
        steps += [(COMBINE, s) for s in at(r)]
    return steps + [(COMBINE, z)]


def layer_kernel(
    layers,
    peers,
    cores,
    cap,
    residual_hbm,
    pool_hbm,
    maps_hbm,
    scale_hbm,
    proj_hbm,
    gain_hbm,
    sg_hbm,
    su_hbm,
    sd_hbm,
    eg_hbm,
    eu_hbm,
    ed_hbm,
    ids_hbm,
    score_hbm,
    out_ref,
    residual,
    pool,
    halo,
    maps,
    scale,
    gain,
    ids,
    score,
    mixed,
    swapped,
    proj,
    gathered,
    metas,
    tables,
    weigh,
    packed,
    arrived,
    results,
    back,
    part,
    landed,
    acc,
    sg,
    su,
    sd,
    eg,
    eu,
    ed,
    w_sem,
    h_sem,
    x_send,
    x_recv,
    z_send,
    z_recv,
    m_send,
    m_recv,
    a_send,
    a_recv,
    b_send,
    b_recv,
    c_send,
    c_recv,
):
    per_layer = peers // cores
    sp = lax.axis_index("sp")
    size_sp = layers * per_layer
    core = lax.axis_index("tp")
    z = sp // per_layer
    q = sp % per_layer
    me = q * cores + core
    blocks, tokens, cols = acc.shape
    width = blocks * cols
    slots = peers * cap
    top = ids.shape[1]
    rows, channels = pool.shape
    group_width = maps.shape[1]
    groups_here = channels // group_width
    f32, bf16 = jnp.float32, jnp.bfloat16

    def in_column(s):
        return (s * per_layer + q, core)

    def in_layer(p):
        return (z * per_layer + p // cores, p % cores)

    def remote(src, dst, send, recv, to):
        return pltpu.make_async_remote_copy(
            src_ref=src,
            dst_ref=dst,
            send_sem=send,
            recv_sem=recv,
            device_id=to,
            device_id_type=pl.DeviceIdType.MESH,
        )

    def tell(to):
        pl.semaphore_signal(
            pltpu.get_barrier_semaphore(), inc=1, device_id=to,
            device_id_type=pl.DeviceIdType.MESH,
        )

    first = pl.multiple_of(core * groups_here, groups_here)
    own_channels = pl.ds(pl.multiple_of(core * channels, channels), channels)
    pairs = (
        (pool_hbm, pool),
        (ids_hbm, ids),
        (score_hbm, score),
        (maps_hbm.at[pl.ds(first, groups_here)], maps),
        (scale_hbm.at[:, own_channels], scale),
        (proj_hbm, proj),
        (residual_hbm, residual),
        (gain_hbm, gain),
        (sg_hbm, sg),
        (su_hbm, su),
        (sd_hbm, sd),
        (eg_hbm.at[0], eg),
        (eu_hbm.at[0], eu),
        (ed_hbm.at[0], ed),
    )
    loads = [pltpu.make_async_copy(a, b, w_sem.at[i]) for i, (a, b) in enumerate(pairs)]
    for load in loads[:5]:
        load.start()
    for o in range(1, layers):
        tell(in_column((z + o) % layers))
    for o in range(1, peers):
        tell(in_layer((me + o) % peers))

    @pl.when(sp > 0)
    def _():
        tell((sp - 1, core))

    for load in loads[5:]:
        load.start()

    loads[1].wait()
    loads[2].wait()
    experts = layers * peers
    ids_now = ids[...]
    score_now = score[...]
    expert_at = lax.broadcasted_iota(jnp.int32, (tokens, experts), 1)
    named = [(ids_now[:, k : k + 1] == expert_at).astype(f32) for k in range(top)]
    named_any = functools.reduce(jnp.add, named).astype(bf16)
    earlier = (
        lax.broadcasted_iota(jnp.int32, (tokens, tokens), 1)
        < lax.broadcasted_iota(jnp.int32, (tokens, tokens), 0)
    ).astype(bf16)
    rank = jnp.dot(earlier, named_any, preferred_element_type=f32)
    shares = score_now / jnp.sum(score_now, axis=1, keepdims=True) * routed_scale
    lane = lax.broadcasted_iota(jnp.int32, (tokens, 128), 1)
    meta = jnp.zeros((tokens, 128), f32)
    for k in range(top):
        position = jnp.sum(rank * named[k], axis=1, keepdims=True)
        slot = ids_now[:, k : k + 1].astype(f32) * cap + position
        meta = jnp.where(lane == k, slot, meta)
        meta = jnp.where(lane == top + k, shares[:, k : k + 1], meta)
    metas[z] = jnp.transpose(meta)[: 2 * top]

    pl.semaphore_wait(
        pltpu.get_barrier_semaphore(),
        layers - 1 + peers - 1 + jnp.where(sp < size_sp - 1, 1, 0),
    )

    def halo_copy():
        return remote(
            pool.at[pl.ds(rows - halo_rows, halo_rows)], halo, h_sem.at[0], h_sem.at[1],
            (jnp.minimum(sp + 1, size_sp - 1), core),
        )

    loads[0].wait()

    @pl.when(sp < size_sp - 1)
    def _():
        halo_copy().start()

    def meta_copy(target, source):
        return remote(
            metas.at[source], metas.at[source], m_send.at[target], m_recv.at[source],
            in_column(target),
        )

    for o in range(1, layers):
        meta_copy((z + o) % layers, z).start()

    def chunk_copy(s, k, side):
        to = jnp.clip(jnp.where(side == 0, z + 1, z - 1), 0, layers - 1)
        return remote(
            gathered.at[s, k], gathered.at[s, k], z_send.at[side, s, k], z_recv.at[s, k],
            in_column(to),
        )

    def pack_copy(s, k, p, source):
        return remote(
            packed.at[s, k, p], arrived.at[s, k, source], a_send.at[s, k, p],
            a_recv.at[s, k, source], in_layer(p),
        )

    def back_copy(s, k, p, source):
        return remote(
            results.at[s, k, p], back.at[s, k, source], b_send.at[s, k, p],
            b_recv.at[s, k, source], in_layer(p),
        )

    def own_pack(s, k):
        return pltpu.make_async_copy(
            packed.at[s, k, me], arrived.at[s, k, me], a_recv.at[s, k, me]
        )

    def own_back(s, k):
        return pltpu.make_async_copy(
            results.at[s, k, me], back.at[s, k, me], b_recv.at[s, k, me]
        )

    def part_copy(s, k, side):
        to = jnp.clip(jnp.where(side == 0, z + 1, z - 1), 0, layers - 1)
        return remote(
            part.at[s, k], landed.at[side, s, k], c_send.at[s, k], c_recv.at[side, s, k],
            in_column(to),
        )

    far_first = sorted(range(1, peers), key=lambda o: (o % cores, -o % 3, o))

    @pl.when(sp == 0)
    def _():
        halo[...] = jnp.zeros(halo.shape, bf16)

    @pl.when(sp > 0)
    def _():
        halo_copy().wait_recv()

    loads[3].wait()
    loads[4].wait()
    half = rows // cores
    place = sp * rows + lax.broadcasted_iota(jnp.int32, (rows, group_width), 0)
    for g in range(groups_here):
        lanes = slice(g * group_width, (g + 1) * group_width)
        own = pool[:, lanes].astype(f32)
        total = jnp.concatenate([halo[:, lanes].astype(f32), own], axis=0)
        span = 1
        while span < windows[g % 4]:
            total = total + pltpu.roll(total, span, 0)
            span = span * 2
        divisor = jnp.minimum(place + 1, span).astype(f32)
        contrast = (total[halo_rows:] / divisor - own).astype(bf16)
        mapped = jnp.dot(contrast, maps[g], preferred_element_type=f32)
        mapped = (mapped * scale[:, lanes]).astype(bf16)
        for c in range(cores):
            mixed[c, :, lanes] = mapped[c * half : (c + 1) * half]

    def swap_copy(p, source):
        return remote(
            mixed.at[p], swapped.at[source], x_send.at[p], x_recv.at[source], (sp, p)
        )

    for o in range(1, cores):
        swap_copy((core + o) % cores, core).start()
    loads[5].wait()
    loads[6].wait()
    loads[7].wait()

    def channels_of(c):
        return pl.ds(pl.multiple_of(c * channels, channels), channels)

    for k in range(blocks):
        lanes = slice(k * cols, (k + 1) * cols)
        acc[k] = residual[:, lanes].astype(f32) + jnp.dot(
            mixed[core], proj[channels_of(core), lanes], preferred_element_type=f32
        )
    squares = jnp.zeros((tokens, 1), f32)
    for o in range(1, cores):
        p = (core + o) % cores
        swap_copy(p, p).wait_recv()
        for k in range(blocks):
            lanes = slice(k * cols, (k + 1) * cols)
            acc[k] = acc[k] + jnp.dot(
                swapped[p], proj[channels_of(p), lanes], preferred_element_type=f32
            )
    for k in range(blocks):
        settled = acc[k].astype(bf16).astype(f32)
        acc[k] = settled
        squares = squares + jnp.sum(settled * settled, axis=1, keepdims=True)
    inverse = lax.rsqrt(squares / width + epsilon)
    for k in range(blocks):
        gathered[z, k] = (acc[k] * inverse * gain[:, k * cols : (k + 1) * cols]).astype(bf16)

        @pl.when(z < layers - 1)
        def _():
            chunk_copy(z, k, 0).start()

        @pl.when(z > 0)
        def _():
            chunk_copy(z, k, 1).start()

    def prepare(s):
        rows_now = metas[s]
        ids_down = lax.broadcasted_iota(jnp.int32, (slots, tokens), 0).astype(f32)
        ids_down = ids_down + (z * slots).astype(f32)
        table = jnp.zeros((slots, tokens), f32)
        value = jnp.zeros((slots, tokens), f32)
        for k in range(top):
            hit = ids_down == rows_now[k : k + 1]
            table = jnp.where(hit, 1.0, table)
            value = jnp.where(hit, rows_now[top + k : top + k + 1], value)
        tables[s] = table.astype(bf16)
        high = value.astype(bf16)
        weigh[s, :, :tokens] = high
        weigh[s, :, tokens:] = (value - high.astype(f32)).astype(bf16)

    def arrive(code):
        r = code // 2

        def one(i, carry):
            side = i % 2
            k = (code % 2) * (blocks // 2) + i // 2
            s = jnp.where(side == 0, z - r, z + r)
            here = jnp.logical_and(s >= 0, s < layers)
            here = jnp.logical_and(here, jnp.logical_or(r > 0, side == 0))
            far = jnp.logical_and(here, r > 0)
            onward = jnp.logical_and(far, jnp.where(side == 0, z < layers - 1, z > 0))
            s = jnp.clip(s, 0, layers - 1)

            @pl.when(jnp.logical_and(far, k == 0))
            def _():
                meta_copy(z, s).wait_recv()

            @pl.when(jnp.logical_and(here, k == 0))
            def _():
                prepare(s)

            @pl.when(far)
            def _():
                chunk_copy(s, k, 0).wait_recv()

            @pl.when(onward)
            def _():
                chunk_copy(s, k, side).start()

            @pl.when(here)
            def _():
                got = jnp.dot(tables[s], gathered[s, k], preferred_element_type=f32)
                packed[s, k] = got.astype(bf16).reshape(peers, cap, cols)
                for o in far_first:
                    pack_copy(s, k, (me + o) % peers, me).start()
                own_pack(s, k).start()

            return carry

        lax.fori_loop(0, 2 * (blocks // 2), one, 0)

    def mlp(tall, w_gate, w_up):
        gate = jnp.dot(tall, w_gate[...], preferred_element_type=f32)
        up = jnp.dot(tall, w_up[...], preferred_element_type=f32)
        return (gate / (1.0 + jnp.exp(-gate)) * up).astype(bf16)

    def expert(s):
        def taken(k, carry):
            for o in range(1, peers):
                p = (me + o) % peers
                pack_copy(s, k, p, p).wait_recv()
            own_pack(s, k).wait()
            return carry

        lax.fori_loop(0, blocks, taken, 0)
        tall = jnp.concatenate(
            [arrived[s, k].reshape(slots, cols) for k in range(blocks)], axis=1
        )
        hidden = mlp(tall, eg, eu)
        for k in range(blocks):
            got = jnp.dot(hidden, ed[:, k * cols : (k + 1) * cols], preferred_element_type=f32)
            results[s, k] = got.astype(bf16).reshape(peers, cap, cols)
            for o in far_first:
                back_copy(s, k, (me + o) % peers, me).start()
            own_back(s, k).start()

    def combine(s):
        below = jnp.logical_and(s >= z, z > 0)
        above = jnp.logical_and(s <= z, z < layers - 1)

        def one(k, carry):
            for o in range(1, peers):
                p = (me + o) % peers
                back_copy(s, k, p, p).wait_recv()
            own_back(s, k).wait()
            both = lax.dot_general(
                weigh[s], back[s, k].reshape(slots, cols), (((0,), (0,)), ((), ())),
                preferred_element_type=f32,
            )
            got = both[:tokens] + both[tokens:]

            @pl.when(below)
            def _():
                part_copy(s, k, 0).wait_recv()

            @pl.when(above)
            def _():
                part_copy(s, k, 1).wait_recv()

            @pl.when(s == z)
            def _():
                total = acc[k] + got
                total = total + jnp.where(below, landed[0, s, k].astype(f32), 0.0)
                total = total + jnp.where(above, landed[1, s, k].astype(f32), 0.0)
                out_ref[:, pl.ds(pl.multiple_of(k * cols, cols), cols)] = total.astype(bf16)

            @pl.when(s > z)
            def _():
                total = got + jnp.where(below, landed[0, s, k].astype(f32), 0.0)
                part[s, k] = total.astype(bf16)
                part_copy(s, k, 0).start()

            @pl.when(s < z)
            def _():
                total = got + jnp.where(above, landed[1, s, k].astype(f32), 0.0)
                part[s, k] = total.astype(bf16)
                part_copy(s, k, 1).start()

            return carry

        lax.fori_loop(0, blocks, one, 0)

    def shared():
        for load in loads[8:11]:
            load.wait()
        tall = jnp.concatenate([gathered[z, k] for k in range(blocks)], axis=1)
        hidden = mlp(tall, sg, su)
        for k in range(blocks):
            acc[k] = acc[k] + jnp.dot(
                hidden, sd[:, k * cols : (k + 1) * cols], preferred_element_type=f32
            )
        for load in loads[11:]:
            load.wait()

    plans = [steps_of(s, layers) for s in range(layers)]
    count = max(len(plan) for plan in plans)
    kinds, values = [], []
    for t in range(count):
        kind, value = jnp.int32(NOP), jnp.int32(0)
        for s, plan in enumerate(plans):
            if t < len(plan):
                kind = jnp.where(z == s, plan[t][0], kind)
                value = jnp.where(z == s, plan[t][1], value)
        kinds.append(kind)
        values.append(value)

    def step(t, carry):
        kind, value = jnp.int32(NOP), jnp.int32(0)
        for i in range(count):
            kind = jnp.where(t == i, kinds[i], kind)
            value = jnp.where(t == i, values[i], value)
        for number, act in (
            (ARRIVE, arrive), (EXPERT, expert), (COMBINE, combine),
        ):
            @pl.when(kind == number)
            def _():
                act(value)

        @pl.when(kind == SHARED)
        def _():
            shared()

        return carry

    lax.fori_loop(0, count, step, 0)

    def drain(i, carry):
        s = i // blocks
        k = i % blocks

        @pl.when(jnp.logical_and(s <= z, z < layers - 1))
        def _():
            chunk_copy(s, k, 0).wait_send()

        @pl.when(jnp.logical_and(s >= z, z > 0))
        def _():
            chunk_copy(s, k, 1).wait_send()

        for o in range(1, peers):
            p = (me + o) % peers
            pack_copy(s, k, p, me).wait_send()
            back_copy(s, k, p, me).wait_send()

        @pl.when(s != z)
        def _():
            part_copy(s, k, 0).wait_send()

        return carry

    lax.fori_loop(0, layers * blocks, drain, 0)
    for o in range(1, layers):
        meta_copy((z + o) % layers, z).wait_send()
    for o in range(1, cores):
        swap_copy((core + o) % cores, core).wait_send()

    @pl.when(sp < size_sp - 1)
    def _():
        halo_copy().wait_send()


def on_device(
    residual,
    pool_input,
    group_maps,
    pool_scale,
    out_proj,
    norm_gain,
    shared_gate,
    shared_up,
    shared_down,
    expert_gate,
    expert_up,
    expert_down,
    expert_ids,
    route_score,
):
    rows, channels = pool_input.shape
    group_width = group_maps.shape[1]
    tokens, top = expert_ids.shape
    width = residual.shape[1]
    size_sp = lax.axis_size("sp")
    cores = lax.axis_size("tp")
    experts = size_sp * cores
    capacity = 3 * tokens * top // (2 * experts)
    cap = -(-capacity // 8) * 8
    layers = layer_count(size_sp)
    peers = experts // layers
    slots = peers * cap
    hidden_width = shared_gate.shape[1]
    expert_width = expert_gate.shape[2]
    cols = min(width, 512)
    blocks = width // cols
    bf16, f32 = jnp.bfloat16, jnp.float32
    dma = pltpu.SemaphoreType.DMA
    routed = (layers, blocks, peers, cap, cols)
    chunks = (layers, blocks, tokens, cols)
    return pl.pallas_call(
        functools.partial(layer_kernel, layers, peers, cores, cap),
        out_shape=jax.ShapeDtypeStruct((tokens, width), bf16),
        in_specs=[pl.BlockSpec(memory_space=pl.ANY)] * 14,
        out_specs=pl.BlockSpec(memory_space=pltpu.VMEM),
        scratch_shapes=[
            pltpu.VMEM((tokens, width), bf16),
            pltpu.VMEM((rows, channels), bf16),
            pltpu.VMEM((halo_rows, channels), bf16),
            pltpu.VMEM((channels // group_width, group_width, group_width), bf16),
            pltpu.VMEM((1, channels), f32),
            pltpu.VMEM((1, width), f32),
            pltpu.VMEM((tokens, top), jnp.int32),
            pltpu.VMEM((tokens, top), f32),
            pltpu.VMEM((cores, rows // cores, channels), bf16),
            pltpu.VMEM((cores, rows // cores, channels), bf16),
            pltpu.VMEM(out_proj.shape, bf16),
            pltpu.VMEM(chunks, bf16),
            pltpu.VMEM((layers, 2 * top, tokens), f32),
            pltpu.VMEM((layers, slots, tokens), bf16),
            pltpu.VMEM((layers, slots, 2 * tokens), bf16),
            pltpu.VMEM(routed, bf16),
            pltpu.VMEM(routed, bf16),
            pltpu.VMEM(routed, bf16),
            pltpu.VMEM(routed, bf16),
            pltpu.VMEM(chunks, bf16),
            pltpu.VMEM((2,) + chunks, bf16),
            pltpu.VMEM((blocks, tokens, cols), f32),
            pltpu.VMEM((width, hidden_width), bf16),
            pltpu.VMEM((width, hidden_width), bf16),
            pltpu.VMEM((hidden_width, width), bf16),
            pltpu.VMEM((width, expert_width), bf16),
            pltpu.VMEM((width, expert_width), bf16),
            pltpu.VMEM((expert_width, width), bf16),
            dma((14,)),
            dma((2,)),
            dma((cores,)),
            dma((cores,)),
            dma((2, layers, blocks)),
            dma((layers, blocks)),
            dma((layers,)),
            dma((layers,)),
            dma((layers, blocks, peers)),
            dma((layers, blocks, peers)),
            dma((layers, blocks, peers)),
            dma((layers, blocks, peers)),
            dma((layers, blocks)),
            dma((2, layers, blocks)),
        ],
        compiler_params=pltpu.CompilerParams(
            collective_id=0, has_side_effects=True, vmem_limit_bytes=60 * 1024 * 1024
        ),
    )(
        residual,
        pool_input,
        group_maps,
        pool_scale.reshape(1, -1),
        out_proj,
        norm_gain.reshape(1, -1),
        shared_gate,
        shared_up,
        shared_down,
        expert_gate,
        expert_up,
        expert_down,
        expert_ids,
        route_score,
    )


def solution(mesh):
    in_specs = (
        P(("sp", "tp"), None),
        P("sp", "tp"),
        P(),
        P(),
        P(),
        P(),
        P(),
        P(),
        P(),
        P(("sp", "tp"), None, None),
        P(("sp", "tp"), None, None),
        P(("sp", "tp"), None, None),
        P(("sp", "tp"), None),
        P(("sp", "tp"), None),
    )
    out_specs = P(("sp", "tp"), None)
    return jax.shard_map(
        on_device, mesh=mesh, in_specs=in_specs, out_specs=out_specs, check_vma=False
    )
```

```python
import functools
import math

import jax
import jax.numpy as jnp
from jax import lax
from jax.experimental import pallas as pl
from jax.experimental.pallas import tpu as pltpu
from jax.sharding import PartitionSpec as P

windows = (2, 4, 8, 16)
epsilon = 1e-06
routed_scale = 2.5
halo_rows = 16


def layer_count(size_sp):
    return max(d for d in range(1, math.isqrt(size_sp) + 1) if size_sp % d == 0)


END = " ".join(
    (
        "a00 a01 a02 a03",
        "a10 a11 a12 a13",
        "a20 a21 e1 b10",
        "a22 a23 a30 s",
        "b11 c10 a31 a32",
        "e2 a33 c11 b20",
        "b21 e3 c20 b30",
        "c21 b31 e0 b32",
        "b33 b22 b23 c30",
        "b00 c31 b12 c32",
        "c33 b13 b01 c22",
        "c23 c12 b02 c00",
        "b03 c13 c01 c02",
        "c03",
    )
)
MIDDLE = " ".join(
    (
        "a00 a01 a02 a03",
        "a10 a11 a12 a13",
        "e1 a20 a21 a22",
        "e0 b10 a23 e2",
        "b20 b00 b21 e3",
        "b01 b30 b31 b22",
        "c20 b32 b33 c21",
        "s c10 b02 c30",
        "b11 b03 c31 b23",
        "c00 c32 c01 c33",
        "c11 c02 b12 c22",
        "c03 b13 c23 c12",
        "c13",
    )
)


def steps_of(z, layers, blocks):
    last = layers - 1
    if (layers, blocks) == (4, 4):
        steps = []
        for word in (END if z in (0, last) else MIDDLE).split():
            numbers = [int(digit) for digit in word[1:]]
            if word[0] in "ebc" and 2 * z > last:
                numbers[0] = last - numbers[0]
            steps.append((word[0], *numbers))
        return steps
    at = lambda r: sorted({s for s in (z - r, z + r) if 0 <= s < layers})
    reach = max(z, last - z)
    span = range(blocks)
    steps = [("a", 0, k) for k in span] + [("s",)]
    for r in range(1, reach + 2):
        if r <= reach:
            steps += [("a", r, k) for k in span]
        for s in at(r - 1):
            steps += [("e", s)] + [("b", s, k) for k in span]
    for r in range(reach, -1, -1):
        steps += [("c", s, k) for s in at(r) for k in span]
    return steps


def code_of(step, layers, blocks):
    area = layers * blocks
    base = {"a": 0, "b": area, "c": 2 * area, "e": 3 * area, "s": 3 * area + layers}[step[0]]
    if len(step) == 3:
        return base + step[1] * blocks + step[2]
    return base + sum(step[1:])


def layer_kernel(
    layers,
    peers,
    cores,
    cap,
    residual_hbm,
    pool_hbm,
    maps_hbm,
    scale_hbm,
    proj_hbm,
    gain_hbm,
    sg_hbm,
    su_hbm,
    sd_hbm,
    eg_hbm,
    eu_hbm,
    ed_hbm,
    ids_hbm,
    score_hbm,
    out_hbm,
    residual,
    pool,
    halo,
    head,
    maps,
    scale,
    gain,
    ids,
    score,
    mixed,
    swapped,
    proj,
    gathered,
    metas,
    tables,
    weigh,
    packed,
    arrived,
    results,
    back,
    part,
    landed,
    acc,
    final,
    sg,
    su,
    sd,
    eg,
    eu,
    ed,
    w_sem,
    o_sem,
    h_send,
    h_recv,
    x_send,
    x_recv,
    z_send,
    z_recv,
    m_send,
    m_recv,
    a_send,
    a_recv,
    b_send,
    b_recv,
    c_send,
    c_recv,
):
    per_layer = peers // cores
    sp = lax.axis_index("sp")
    size_sp = layers * per_layer
    core = lax.axis_index("tp")
    z = sp // per_layer
    q = sp % per_layer
    me = q * cores + core
    blocks, tokens, cols = acc.shape
    width = blocks * cols
    slots = peers * cap
    top = ids.shape[0]
    rows, channels = pool.shape
    group_width = maps.shape[1]
    groups_here = channels // group_width
    area = layers * blocks
    f32, bf16 = jnp.float32, jnp.bfloat16

    def in_column(s):
        return (s * per_layer + q, core)

    def in_layer(p):
        return (z * per_layer + p // cores, p % cores)

    def remote(src, dst, send, recv, to):
        return pltpu.make_async_remote_copy(
            src_ref=src,
            dst_ref=dst,
            send_sem=send,
            recv_sem=recv,
            device_id=to,
            device_id_type=pl.DeviceIdType.MESH,
        )

    def tell(to):
        pl.semaphore_signal(
            pltpu.get_barrier_semaphore(), inc=1, device_id=to,
            device_id_type=pl.DeviceIdType.MESH,
        )

    pairs = (
        (pool_hbm, pool),
        (ids_hbm, ids),
        (score_hbm, score),
        (maps_hbm, maps),
        (scale_hbm, scale),
        (proj_hbm, proj),
        (residual_hbm, residual),
        (gain_hbm, gain),
        (sg_hbm, sg),
        (su_hbm, su),
        (sd_hbm, sd),
        (eg_hbm.at[0], eg),
        (eu_hbm.at[0], eu),
        (ed_hbm.at[0], ed),
    )
    loads = [pltpu.make_async_copy(a, b, w_sem.at[i]) for i, (a, b) in enumerate(pairs)]
    for load in loads[:5]:
        load.start()
    for o in range(1, layers):
        tell(in_column((z + o) % layers))
    for o in range(1, peers):
        tell(in_layer((me + o) % peers))

    takes_halo = jnp.logical_and(sp > 0, core == 0)
    gives_halo = sp < size_sp - 1

    @pl.when(takes_halo)
    def _():
        for c in range(cores):
            tell((sp - 1, c))

    for load in loads[5:8]:
        load.start()

    loads[1].wait()
    loads[2].wait()
    experts = layers * peers
    ids_now = ids[...]
    score_now = score[...]
    expert_at = lax.broadcasted_iota(jnp.int32, (experts, tokens), 0)
    named = [(ids_now[k : k + 1] == expert_at).astype(f32) for k in range(top)]
    named_any = functools.reduce(jnp.add, named).astype(bf16)
    earlier = (
        lax.broadcasted_iota(jnp.int32, (tokens, tokens), 0)
        < lax.broadcasted_iota(jnp.int32, (tokens, tokens), 1)
    ).astype(bf16)
    rank = jnp.dot(named_any, earlier, preferred_element_type=f32)
    shares = score_now / jnp.sum(score_now, axis=0, keepdims=True) * routed_scale
    slot = [
        ids_now[k : k + 1].astype(f32) * cap + jnp.sum(rank * named[k], axis=0, keepdims=True)
        for k in range(top)
    ]
    metas[z] = jnp.concatenate(slot + [shares], axis=0)

    half = rows // cores

    def mix(before, own, start, c):
        place = start + lax.broadcasted_iota(jnp.int32, (own.shape[0], group_width), 0)
        out = []
        for g in range(groups_here):
            lanes = slice(g * group_width, (g + 1) * group_width)
            here = own[:, lanes]
            total = jnp.concatenate([before[:, lanes], here], axis=0)
            span = 1
            while span < windows[g % 4]:
                total = total + pltpu.roll(total, span, 0)
                span = span * 2
            divisor = jnp.minimum(place + 1, span).astype(f32)
            contrast = (total[halo_rows:] / divisor - here).astype(bf16)
            group = c * groups_here + g
            mapped = jnp.dot(contrast, maps[group], preferred_element_type=f32)
            out.append((mapped * scale[group]).astype(bf16))
        return jnp.concatenate(out, axis=1)

    for i in (0, 3, 4):
        loads[i].wait()
    for c in range(cores):
        start = c * half
        before = pool[max(start - halo_rows, 0) : max(start, halo_rows)].astype(f32)
        if c == 0:
            before = jnp.zeros_like(before)
        mixed[c] = mix(before, pool[start : start + half].astype(f32), sp * rows + start, core)

    pl.semaphore_wait(
        pltpu.get_barrier_semaphore(),
        layers - 1 + peers - 1 + jnp.where(gives_halo, 1, 0),
    )

    def halo_copy(source):
        return remote(
            pool.at[pl.ds(rows - halo_rows, halo_rows)], halo.at[source], h_send.at[0],
            h_recv.at[0, source], (jnp.minimum(sp + 1, size_sp - 1), 0),
        )

    def head_copy(source):
        return remote(
            pool.at[pl.ds(0, halo_rows)], head.at[source], h_send.at[1],
            h_recv.at[1, source], (sp, 0),
        )

    def swap_copy(p, source):
        return remote(
            mixed.at[p], swapped.at[source], x_send.at[p], x_recv.at[source], (sp, p)
        )

    @pl.when(gives_halo)
    def _():
        halo_copy(core).start()

    for o in range(1, cores):
        swap_copy((core + o) % cores, core).start()

    gives_head = jnp.logical_and(sp > 0, core > 0)

    @pl.when(gives_head)
    def _():
        head_copy(core).start()

    def meta_copy(target, source):
        return remote(
            metas.at[source], metas.at[source], m_send.at[target], m_recv.at[source],
            in_column(target),
        )

    for o in range(1, layers):
        meta_copy((z + o) % layers, z).start()
    for load in loads[8:11]:
        load.start()

    def neighbour(side):
        return in_column(jnp.clip(jnp.where(side == 0, z + 1, z - 1), 0, layers - 1))

    def chunk_copy(s, k, side):
        return remote(
            gathered.at[s, k], gathered.at[s, k], z_send.at[side, s], z_recv.at[s, k],
            neighbour(side),
        )

    def pack_copy(s, k, p, source):
        return remote(
            packed.at[s, k, p], arrived.at[s, k, source], a_send.at[s],
            a_recv.at[s], in_layer(p),
        )

    def back_copy(s, k, p, source):
        return remote(
            results.at[s, k, p], back.at[s, k, source], b_send.at[s],
            b_recv.at[s, k], in_layer(p),
        )

    def own_pack(s, k):
        return pltpu.make_async_copy(
            packed.at[s, k, me], arrived.at[s, k, me], a_recv.at[s]
        )

    def own_back(s, k):
        return pltpu.make_async_copy(
            results.at[s, k, me], back.at[s, k, me], b_recv.at[s, k]
        )

    def part_copy(s, k, side):
        slot = jnp.where(jnp.logical_and(side == 1, s == z - 1), layers, s)
        return remote(
            part.at[s, k], landed.at[slot, k], c_send.at[s], c_recv.at[slot, k],
            neighbour(side),
        )

    def wait_bytes(ref, sem):
        pltpu.make_async_copy(ref, ref, sem).wait()

    far_first = sorted(range(1, peers), key=lambda o: (o % cores, -o % 3, o))

    for load in loads[11:]:
        load.start()
    for o in range(1, cores):
        p = (core + o) % cores
        swap_copy(p, p).wait_recv()

    @pl.when(takes_halo)
    def _():
        for c in range(cores):
            halo_copy(c).wait_recv()
            own = pool[:halo_rows]
            if c > 0:
                head_copy(c).wait_recv()
                own = head[c]
            fixed = mix(halo[c].astype(f32), own.astype(f32), sp * rows, c)
            if c == 0:
                mixed[0, :halo_rows] = fixed
            else:
                swapped[c, :halo_rows] = fixed

    for load in loads[5:8]:
        load.wait()

    def channels_of(c):
        return pl.ds(pl.multiple_of(c * channels, channels), channels)

    for k in range(blocks):
        lanes = slice(k * cols, (k + 1) * cols)
        total = residual[:, lanes].astype(f32) + jnp.dot(
            mixed[core], proj[channels_of(core), lanes], preferred_element_type=f32
        )
        for o in range(1, cores):
            p = (core + o) % cores
            total = total + jnp.dot(
                swapped[p], proj[channels_of(p), lanes], preferred_element_type=f32
            )
        acc[k] = total
    squares = jnp.zeros((tokens, 1), f32)
    for k in range(blocks):
        settled = acc[k].astype(bf16).astype(f32)
        acc[k] = settled
        squares = squares + jnp.sum(settled * settled, axis=1, keepdims=True)
    inverse = lax.rsqrt(squares / width + epsilon)
    for k in range(blocks):
        gathered[z, k] = (acc[k] * inverse * gain[:, k * cols : (k + 1) * cols]).astype(bf16)

        @pl.when(z < layers - 1)
        def _():
            chunk_copy(z, k, 0).start()

        @pl.when(z > 0)
        def _():
            chunk_copy(z, k, 1).start()

    def prepare(s):
        rows_now = metas[s]
        ids_down = lax.broadcasted_iota(jnp.int32, (slots, tokens), 0).astype(f32)
        ids_down = ids_down + (z * slots).astype(f32)
        table = jnp.zeros((slots, tokens), f32)
        value = jnp.zeros((slots, tokens), f32)
        for k in range(top):
            hit = ids_down == rows_now[k : k + 1]
            table = jnp.where(hit, 1.0, table)
            value = jnp.where(hit, rows_now[top + k : top + k + 1], value)
        tables[s] = table.astype(bf16)
        high = value.astype(bf16)
        weigh[s, :, :tokens] = high
        weigh[s, :, tokens:] = (value - high.astype(f32)).astype(bf16)

    def arrive(r, k):
        def one(side, carry):
            s = jnp.where(side == 0, z - r, z + r)
            here = jnp.logical_and(s >= 0, s < layers)
            here = jnp.logical_and(here, jnp.logical_or(r > 0, side == 0))
            far = jnp.logical_and(here, r > 0)
            onward = jnp.logical_and(far, jnp.where(side == 0, z < layers - 1, z > 0))
            s = jnp.clip(s, 0, layers - 1)

            @pl.when(far)
            def _():
                chunk_copy(s, k, 0).wait_recv()

            @pl.when(onward)
            def _():
                chunk_copy(s, k, side).start()

            @pl.when(jnp.logical_and(far, k == 0))
            def _():
                meta_copy(z, s).wait_recv()

            @pl.when(jnp.logical_and(here, k == 0))
            def _():
                prepare(s)

            @pl.when(here)
            def _():
                got = jnp.dot(tables[s], gathered[s, k], preferred_element_type=f32)
                packed[s, k] = got.astype(bf16).reshape(peers, cap, cols)
                for o in far_first:
                    pack_copy(s, k, (me + o) % peers, me).start()
                own_pack(s, k).start()

            return carry

        lax.fori_loop(0, 2, one, 0)

    def mlp(tall, w_gate, w_up):
        gate = jnp.dot(tall, w_gate[...], preferred_element_type=f32)
        up = jnp.dot(tall, w_up[...], preferred_element_type=f32)
        return (gate / (1.0 + jnp.exp(-gate)) * up).astype(bf16)

    def expert(s):
        wait_bytes(arrived.at[s], a_recv.at[s])
        tall = jnp.concatenate(
            [arrived[s, k].reshape(slots, cols) for k in range(blocks)], axis=1
        )
        hidden = mlp(tall, eg, eu)
        for k in range(blocks):
            got = jnp.dot(hidden, ed[:, k * cols : (k + 1) * cols], preferred_element_type=f32)
            results[s, k] = got.astype(bf16).reshape(peers, cap, cols)

    def give_back(s, k):
        for o in far_first:
            back_copy(s, k, (me + o) % peers, me).start()
        own_back(s, k).start()

    def out_copy(k):
        lanes = pl.ds(pl.multiple_of(k * cols, cols), cols)
        return pltpu.make_async_copy(final.at[k], out_hbm.at[:, lanes], o_sem.at[k])

    def combine(s, k):
        below = jnp.logical_and(s >= z, z > 0)
        above = jnp.logical_and(s <= z, z < layers - 1)
        over = jnp.where(s == z, layers, s)
        wait_bytes(back.at[s, k], b_recv.at[s, k])
        both = lax.dot_general(
            weigh[s], back[s, k].reshape(slots, cols), (((0,), (0,)), ((), ())),
            preferred_element_type=f32,
        )
        got = both[:tokens] + both[tokens:]

        @pl.when(below)
        def _():
            wait_bytes(landed.at[s, k], c_recv.at[s, k])

        @pl.when(above)
        def _():
            wait_bytes(landed.at[over, k], c_recv.at[over, k])

        got = got + jnp.where(below, landed[s, k].astype(f32), 0.0)
        got = got + jnp.where(above, landed[over, k].astype(f32), 0.0)

        @pl.when(s == z)
        def _():
            final[k] = (acc[k] + got).astype(bf16)
            out_copy(k).start()

        @pl.when(s != z)
        def _():
            part[s, k] = got.astype(bf16)
            part_copy(s, k, jnp.where(s > z, 0, 1)).start()

    def shared():
        for load in loads[8:11]:
            load.wait()
        tall = jnp.concatenate([gathered[z, k] for k in range(blocks)], axis=1)
        hidden = mlp(tall, sg, su)
        for k in range(blocks):
            acc[k] = acc[k] + jnp.dot(
                hidden, sd[:, k * cols : (k + 1) * cols], preferred_element_type=f32
            )

    plans = [
        [code_of(step, layers, blocks) for step in steps_of(s, layers, blocks)]
        for s in range(layers)
    ]
    nothing = 3 * area + layers + 1
    base = 1 << nothing.bit_length()
    per_word = 30 // nothing.bit_length()
    count = -(-max(len(plan) for plan in plans) // per_word)
    words = []
    for i in range(count):
        word = jnp.int32(0)
        for s, plan in enumerate(plans):
            codes = plan[i * per_word : (i + 1) * per_word]
            codes = codes + [nothing] * (per_word - len(codes))
            packed_codes = sum(code * base**j for j, code in enumerate(codes))
            word = jnp.where(z == s, packed_codes, word)
        words.append(word)

    def act(code):
        number = code % area
        s = number // blocks
        k = number % blocks

        @pl.when(code < area)
        def _():
            arrive(s, k)

        @pl.when(code == 2 * blocks - 1)
        def _():
            for load in loads[11:]:
                load.wait()

        @pl.when(jnp.logical_and(code >= area, code < 2 * area))
        def _():
            give_back(s, k)

        @pl.when(jnp.logical_and(code >= 2 * area, code < 3 * area))
        def _():
            combine(s, k)

        @pl.when(jnp.logical_and(code >= 3 * area, code < 3 * area + layers))
        def _():
            expert(code - 3 * area)

        @pl.when(code == 3 * area + layers)
        def _():
            shared()

    def several(i, carry):
        word = words[0]
        for j in range(1, count):
            word = jnp.where(i == j, words[j], word)

        def single(j, word):
            act(word % base)
            return word // base

        lax.fori_loop(0, per_word, single, word)
        return carry

    lax.fori_loop(0, count, several, 0)

    def drain(s, carry):
        @pl.when(jnp.logical_and(s <= z, z < layers - 1))
        def _():
            wait_bytes(gathered.at[s], z_send.at[0, s])

        @pl.when(jnp.logical_and(s >= z, z > 0))
        def _():
            wait_bytes(gathered.at[s], z_send.at[1, s])

        wait_bytes(packed.at[s, :, pl.ds(1, peers - 1)], a_send.at[s])
        wait_bytes(results.at[s, :, pl.ds(1, peers - 1)], b_send.at[s])

        @pl.when(s != z)
        def _():
            wait_bytes(part.at[s], c_send.at[s])

        return carry

    lax.fori_loop(0, layers, drain, 0)
    for o in range(1, layers):
        meta_copy((z + o) % layers, z).wait_send()
    for o in range(1, cores):
        swap_copy((core + o) % cores, core).wait_send()

    @pl.when(gives_halo)
    def _():
        halo_copy(core).wait_send()

    @pl.when(gives_head)
    def _():
        head_copy(core).wait_send()

    for k in range(blocks):
        out_copy(k).wait()


def on_device(
    residual,
    pool_input,
    group_maps,
    pool_scale,
    out_proj,
    norm_gain,
    shared_gate,
    shared_up,
    shared_down,
    expert_gate,
    expert_up,
    expert_down,
    expert_ids,
    route_score,
):
    rows, channels = pool_input.shape
    group_width = group_maps.shape[1]
    tokens, top = expert_ids.shape
    width = residual.shape[1]
    size_sp = lax.axis_size("sp")
    cores = lax.axis_size("tp")
    experts = size_sp * cores
    capacity = 3 * tokens * top // (2 * experts)
    cap = -(-capacity // 8) * 8
    layers = layer_count(size_sp)
    peers = experts // layers
    slots = peers * cap
    hidden_width = shared_gate.shape[1]
    expert_width = expert_gate.shape[2]
    cols = min(width, 512)
    blocks = width // cols
    bf16, f32 = jnp.bfloat16, jnp.float32
    dma = pltpu.SemaphoreType.DMA
    routed = (layers, blocks, peers, cap, cols)
    chunks = (layers, blocks, tokens, cols)
    return pl.pallas_call(
        functools.partial(layer_kernel, layers, peers, cores, cap),
        out_shape=jax.ShapeDtypeStruct((tokens, width), bf16),
        in_specs=[pl.BlockSpec(memory_space=pltpu.HBM)] * 14,
        out_specs=pl.BlockSpec(memory_space=pltpu.HBM),
        scratch_shapes=[
            pltpu.VMEM((tokens, width), bf16),
            pltpu.VMEM((rows, channels), bf16),
            pltpu.VMEM((cores, halo_rows, channels), bf16),
            pltpu.VMEM((cores, halo_rows, channels), bf16),
            pltpu.VMEM(group_maps.shape, bf16),
            pltpu.VMEM((group_maps.shape[0], 1, group_width), f32),
            pltpu.VMEM((1, width), f32),
            pltpu.VMEM((top, tokens), jnp.int32),
            pltpu.VMEM((top, tokens), f32),
            pltpu.VMEM((cores, rows // cores, channels), bf16),
            pltpu.VMEM((cores, rows // cores, channels), bf16),
            pltpu.VMEM(out_proj.shape, bf16),
            pltpu.VMEM(chunks, bf16),
            pltpu.VMEM((layers, 2 * top, tokens), f32),
            pltpu.VMEM((layers, slots, tokens), bf16),
            pltpu.VMEM((layers, slots, 2 * tokens), bf16),
            pltpu.VMEM(routed, bf16),
            pltpu.VMEM(routed, bf16),
            pltpu.VMEM(routed, bf16),
            pltpu.VMEM(routed, bf16),
            pltpu.VMEM(chunks, bf16),
            pltpu.VMEM((layers + 1, blocks, tokens, cols), bf16),
            pltpu.VMEM((blocks, tokens, cols), f32),
            pltpu.VMEM((blocks, tokens, cols), bf16),
            pltpu.VMEM((width, hidden_width), bf16),
            pltpu.VMEM((width, hidden_width), bf16),
            pltpu.VMEM((hidden_width, width), bf16),
            pltpu.VMEM((width, expert_width), bf16),
            pltpu.VMEM((width, expert_width), bf16),
            pltpu.VMEM((expert_width, width), bf16),
            dma((14,)),
            dma((blocks,)),
            dma((2,)),
            dma((2, cores)),
            dma((cores,)),
            dma((cores,)),
            dma((2, layers)),
            dma((layers, blocks)),
            dma((layers,)),
            dma((layers,)),
            dma((layers,)),
            dma((layers,)),
            dma((layers,)),
            dma((layers, blocks)),
            dma((layers,)),
            dma((layers + 1, blocks)),
        ],
        compiler_params=pltpu.CompilerParams(
            collective_id=0, has_side_effects=True, vmem_limit_bytes=56 * 1024 * 1024
        ),
    )(
        residual,
        pool_input,
        group_maps,
        pool_scale.reshape(-1, 1, group_width),
        out_proj,
        norm_gain.reshape(1, -1),
        shared_gate,
        shared_up,
        shared_down,
        expert_gate,
        expert_up,
        expert_down,
        expert_ids.T,
        route_score.T,
    )


def solution(mesh):
    in_specs = (
        P(("sp", "tp"), None),
        P("sp", "tp"),
        P(),
        P(),
        P(),
        P(),
        P(),
        P(),
        P(),
        P(("sp", "tp"), None, None),
        P(("sp", "tp"), None, None),
        P(("sp", "tp"), None, None),
        P(("sp", "tp"), None),
        P(("sp", "tp"), None),
    )
    out_specs = P(("sp", "tp"), None)
    return jax.shard_map(
        on_device, mesh=mesh, in_specs=in_specs, out_specs=out_specs, check_vma=False
    )
```

```python
import functools
import math

import jax
import jax.numpy as jnp
from jax import lax
from jax.experimental import pallas as pl
from jax.experimental.pallas import tpu as pltpu
from jax.sharding import PartitionSpec as P

windows = (2, 4, 8, 16)
epsilon = 1e-06
routed_scale = 2.5
halo_rows = 16


def layer_count(size_sp):
    return max(d for d in range(1, math.isqrt(size_sp) + 1) if size_sp % d == 0)


END = " ".join(
    (
        "a00 a01 a02 a03",
        "a10 a11 a12 a13",
        "a20 a21 e1 b10",
        "a22 a23 a30 s",
        "b11 c10 a31 a32",
        "e2 a33 c11 b20",
        "b21 e3 c20 b30",
        "c21 b31 e0 b32",
        "b33 b22 b23 c30",
        "b00 c31 b12 c32",
        "c33 b13 b01 c22",
        "c23 c12 b02 c00",
        "b03 c13 c01 c02",
        "c03",
    )
)
MIDDLE = " ".join(
    (
        "a00 a01 a02 a03",
        "a10 a11 a12 a13",
        "e1 a20 a21 a22",
        "e0 b10 a23 e2",
        "b20 b00 b21 e3",
        "b01 b30 b31 b22",
        "c20 b32 b33 c21",
        "s c10 b02 c30",
        "b11 b03 c31 b23",
        "c00 c32 c01 c33",
        "c11 c02 b12 c22",
        "c03 b13 c23 c12",
        "c13",
    )
)


def steps_of(z, layers, blocks):
    last = layers - 1
    if (layers, blocks) == (4, 4):
        steps = []
        for word in (END if z in (0, last) else MIDDLE).split():
            numbers = [int(digit) for digit in word[1:]]
            if word[0] in "ebc" and 2 * z > last:
                numbers[0] = last - numbers[0]
            steps.append((word[0], *numbers))
        return steps
    at = lambda r: sorted({s for s in (z - r, z + r) if 0 <= s < layers})
    reach = max(z, last - z)
    span = range(blocks)
    steps = [("a", 0, k) for k in span] + [("s",)]
    for r in range(1, reach + 2):
        if r <= reach:
            steps += [("a", r, k) for k in span]
        for s in at(r - 1):
            steps += [("e", s)] + [("b", s, k) for k in span]
    for r in range(reach, -1, -1):
        steps += [("c", s, k) for s in at(r) for k in span]
    return steps


def code_of(step, layers, blocks):
    area = layers * blocks
    base = {"a": 0, "b": area, "c": 2 * area, "e": 3 * area, "s": 3 * area + layers}[step[0]]
    if len(step) == 3:
        return base + step[1] * blocks + step[2]
    return base + sum(step[1:])


def layer_kernel(
    layers,
    peers,
    cores,
    cap,
    residual_hbm,
    pool_hbm,
    maps_hbm,
    scale_hbm,
    proj_hbm,
    gain_hbm,
    sg_hbm,
    su_hbm,
    sd_hbm,
    eg_hbm,
    eu_hbm,
    ed_hbm,
    ids_hbm,
    score_hbm,
    out_ref,
    residual,
    pool,
    halo,
    head,
    maps,
    scale,
    gain,
    ids,
    score,
    mixed,
    swapped,
    proj,
    gathered,
    metas,
    tables,
    weigh,
    packed,
    arrived,
    results,
    back,
    part,
    landed,
    acc,
    sg,
    su,
    sd,
    eg,
    eu,
    ed,
    w_sem,
    h_send,
    h_recv,
    x_send,
    x_recv,
    z_send,
    z_recv,
    m_send,
    m_recv,
    a_send,
    a_recv,
    b_send,
    b_recv,
    c_send,
    c_recv,
):
    per_layer = peers // cores
    sp = lax.axis_index("sp")
    size_sp = layers * per_layer
    core = lax.axis_index("tp")
    z = sp // per_layer
    q = sp % per_layer
    me = q * cores + core
    blocks, tokens, cols = acc.shape
    width = blocks * cols
    slots = peers * cap
    top = ids.shape[0]
    rows, channels = pool.shape
    group_width = maps.shape[1]
    groups_here = channels // group_width
    area = layers * blocks
    f32, bf16 = jnp.float32, jnp.bfloat16

    def in_column(s):
        return (s * per_layer + q, core)

    def in_layer(p):
        return (z * per_layer + p // cores, p % cores)

    def remote(src, dst, send, recv, to):
        return pltpu.make_async_remote_copy(
            src_ref=src,
            dst_ref=dst,
            send_sem=send,
            recv_sem=recv,
            device_id=to,
            device_id_type=pl.DeviceIdType.MESH,
        )

    def tell(to):
        pl.semaphore_signal(
            pltpu.get_barrier_semaphore(), inc=1, device_id=to,
            device_id_type=pl.DeviceIdType.MESH,
        )

    pairs = (
        (pool_hbm, pool),
        (ids_hbm, ids),
        (score_hbm, score),
        (maps_hbm, maps),
        (scale_hbm, scale),
        (proj_hbm, proj),
        (residual_hbm, residual),
        (gain_hbm, gain),
        (sg_hbm, sg),
        (su_hbm, su),
        (sd_hbm, sd),
        (eg_hbm.at[0], eg),
        (eu_hbm.at[0], eu),
        (ed_hbm.at[0], ed),
    )
    loads = [pltpu.make_async_copy(a, b, w_sem.at[i]) for i, (a, b) in enumerate(pairs)]
    for load in loads[:5]:
        load.start()
    for o in range(1, layers):
        tell(in_column((z + o) % layers))
    for o in range(1, peers):
        tell(in_layer((me + o) % peers))

    takes_halo = jnp.logical_and(sp > 0, core == 0)
    gives_halo = sp < size_sp - 1

    @pl.when(takes_halo)
    def _():
        for c in range(cores):
            tell((sp - 1, c))

    for load in loads[5:8]:
        load.start()

    loads[1].wait()
    loads[2].wait()
    experts = layers * peers
    ids_now = ids[...]
    score_now = score[...]
    expert_at = lax.broadcasted_iota(jnp.int32, (experts, tokens), 0)
    named = [(ids_now[k : k + 1] == expert_at).astype(f32) for k in range(top)]
    named_any = functools.reduce(jnp.add, named).astype(bf16)
    earlier = (
        lax.broadcasted_iota(jnp.int32, (tokens, tokens), 0)
        < lax.broadcasted_iota(jnp.int32, (tokens, tokens), 1)
    ).astype(bf16)
    rank = jnp.dot(named_any, earlier, preferred_element_type=f32)
    shares = score_now / jnp.sum(score_now, axis=0, keepdims=True) * routed_scale
    slot = [
        ids_now[k : k + 1].astype(f32) * cap + jnp.sum(rank * named[k], axis=0, keepdims=True)
        for k in range(top)
    ]
    metas[z] = jnp.concatenate(slot + [shares], axis=0)

    half = rows // cores

    def mix(before, own, start, c):
        place = start + lax.broadcasted_iota(jnp.int32, (own.shape[0], group_width), 0)
        out = []
        for g in range(groups_here):
            lanes = slice(g * group_width, (g + 1) * group_width)
            here = own[:, lanes]
            total = jnp.concatenate([before[:, lanes], here], axis=0)
            span = 1
            while span < windows[g % 4]:
                total = total + pltpu.roll(total, span, 0)
                span = span * 2
            divisor = jnp.minimum(place + 1, span).astype(f32)
            contrast = (total[halo_rows:] / divisor - here).astype(bf16)
            group = c * groups_here + g
            mapped = jnp.dot(contrast, maps[group], preferred_element_type=f32)
            out.append((mapped * scale[group]).astype(bf16))
        return jnp.concatenate(out, axis=1)

    for i in (0, 3, 4):
        loads[i].wait()
    for c in range(cores):
        start = c * half
        before = pool[max(start - halo_rows, 0) : max(start, halo_rows)].astype(f32)
        if c == 0:
            before = jnp.zeros_like(before)
        mixed[c] = mix(before, pool[start : start + half].astype(f32), sp * rows + start, core)

    pl.semaphore_wait(
        pltpu.get_barrier_semaphore(),
        layers - 1 + peers - 1 + jnp.where(gives_halo, 1, 0),
    )

    def halo_copy(source):
        return remote(
            pool.at[pl.ds(rows - halo_rows, halo_rows)], halo.at[source], h_send.at[0],
            h_recv.at[0, source], (jnp.minimum(sp + 1, size_sp - 1), 0),
        )

    def head_copy(source):
        return remote(
            pool.at[pl.ds(0, halo_rows)], head.at[source], h_send.at[1],
            h_recv.at[1, source], (sp, 0),
        )

    def swap_copy(p, source):
        return remote(
            mixed.at[p], swapped.at[source], x_send.at[p], x_recv.at[source], (sp, p)
        )

    @pl.when(gives_halo)
    def _():
        halo_copy(core).start()

    for o in range(1, cores):
        swap_copy((core + o) % cores, core).start()

    gives_head = jnp.logical_and(sp > 0, core > 0)

    @pl.when(gives_head)
    def _():
        head_copy(core).start()

    def meta_copy(target, source):
        return remote(
            metas.at[source], metas.at[source], m_send.at[target], m_recv.at[source],
            in_column(target),
        )

    for o in range(1, layers):
        meta_copy((z + o) % layers, z).start()
    for load in loads[8:11]:
        load.start()

    def neighbour(side):
        return in_column(jnp.clip(jnp.where(side == 0, z + 1, z - 1), 0, layers - 1))

    def chunk_copy(s, k, side):
        return remote(
            gathered.at[s, k], gathered.at[s, k], z_send.at[side, s], z_recv.at[s, k],
            neighbour(side),
        )

    def pack_copy(s, k, p, source):
        return remote(
            packed.at[s, k, p], arrived.at[s, k, source], a_send.at[s],
            a_recv.at[s], in_layer(p),
        )

    def back_copy(s, k, p, source):
        return remote(
            results.at[s, k, p], back.at[s, k, source], b_send.at[s],
            b_recv.at[s, k], in_layer(p),
        )

    def own_pack(s, k):
        return pltpu.make_async_copy(
            packed.at[s, k, me], arrived.at[s, k, me], a_recv.at[s]
        )

    def own_back(s, k):
        return pltpu.make_async_copy(
            results.at[s, k, me], back.at[s, k, me], b_recv.at[s, k]
        )

    def part_copy(s, k, side):
        slot = jnp.where(jnp.logical_and(side == 1, s == z - 1), layers, s)
        return remote(
            part.at[s, k], landed.at[slot, k], c_send.at[s], c_recv.at[slot, k],
            neighbour(side),
        )

    def wait_bytes(ref, sem):
        pltpu.make_async_copy(ref, ref, sem).wait()

    far_first = sorted(range(1, peers), key=lambda o: (o % cores, -o % 3, o))

    for load in loads[11:]:
        load.start()
    for o in range(1, cores):
        p = (core + o) % cores
        swap_copy(p, p).wait_recv()

    @pl.when(takes_halo)
    def _():
        for c in range(cores):
            halo_copy(c).wait_recv()
            own = pool[:halo_rows]
            if c > 0:
                head_copy(c).wait_recv()
                own = head[c]
            fixed = mix(halo[c].astype(f32), own.astype(f32), sp * rows, c)
            if c == 0:
                mixed[0, :halo_rows] = fixed
            else:
                swapped[c, :halo_rows] = fixed

    for load in loads[5:8]:
        load.wait()

    def channels_of(c):
        return pl.ds(pl.multiple_of(c * channels, channels), channels)

    for k in range(blocks):
        lanes = slice(k * cols, (k + 1) * cols)
        total = residual[:, lanes].astype(f32) + jnp.dot(
            mixed[core], proj[channels_of(core), lanes], preferred_element_type=f32
        )
        for o in range(1, cores):
            p = (core + o) % cores
            total = total + jnp.dot(
                swapped[p], proj[channels_of(p), lanes], preferred_element_type=f32
            )
        acc[k] = total
    squares = jnp.zeros((tokens, 1), f32)
    for k in range(blocks):
        settled = acc[k].astype(bf16).astype(f32)
        acc[k] = settled
        squares = squares + jnp.sum(settled * settled, axis=1, keepdims=True)
    inverse = lax.rsqrt(squares / width + epsilon)
    for k in range(blocks):
        gathered[z, k] = (acc[k] * inverse * gain[:, k * cols : (k + 1) * cols]).astype(bf16)

        @pl.when(z < layers - 1)
        def _():
            chunk_copy(z, k, 0).start()

        @pl.when(z > 0)
        def _():
            chunk_copy(z, k, 1).start()

    def prepare(s):
        rows_now = metas[s]
        ids_down = lax.broadcasted_iota(jnp.int32, (slots, tokens), 0).astype(f32)
        ids_down = ids_down + (z * slots).astype(f32)
        table = jnp.zeros((slots, tokens), f32)
        value = jnp.zeros((slots, tokens), f32)
        for k in range(top):
            hit = ids_down == rows_now[k : k + 1]
            table = jnp.where(hit, 1.0, table)
            value = jnp.where(hit, rows_now[top + k : top + k + 1], value)
        tables[s] = table.astype(bf16)
        high = value.astype(bf16)
        weigh[s, :, :tokens] = high
        weigh[s, :, tokens:] = (value - high.astype(f32)).astype(bf16)

    def arrive(r, k):
        def one(side, carry):
            s = jnp.where(side == 0, z - r, z + r)
            here = jnp.logical_and(s >= 0, s < layers)
            here = jnp.logical_and(here, jnp.logical_or(r > 0, side == 0))
            far = jnp.logical_and(here, r > 0)
            onward = jnp.logical_and(far, jnp.where(side == 0, z < layers - 1, z > 0))
            s = jnp.clip(s, 0, layers - 1)

            @pl.when(far)
            def _():
                chunk_copy(s, k, 0).wait_recv()

            @pl.when(onward)
            def _():
                chunk_copy(s, k, side).start()

            @pl.when(jnp.logical_and(far, k == 0))
            def _():
                meta_copy(z, s).wait_recv()

            @pl.when(jnp.logical_and(here, k == 0))
            def _():
                prepare(s)

            @pl.when(here)
            def _():
                got = jnp.dot(tables[s], gathered[s, k], preferred_element_type=f32)
                packed[s, k] = got.astype(bf16).reshape(peers, cap, cols)
                for o in far_first:
                    pack_copy(s, k, (me + o) % peers, me).start()
                own_pack(s, k).start()

            return carry

        lax.fori_loop(0, 2, one, 0)

    def mlp(tall, w_gate, w_up):
        gate = jnp.dot(tall, w_gate[...], preferred_element_type=f32)
        up = jnp.dot(tall, w_up[...], preferred_element_type=f32)
        return (gate / (1.0 + jnp.exp(-gate)) * up).astype(bf16)

    def expert(s):
        wait_bytes(arrived.at[s], a_recv.at[s])
        tall = jnp.concatenate(
            [arrived[s, k].reshape(slots, cols) for k in range(blocks)], axis=1
        )
        hidden = mlp(tall, eg, eu)
        for k in range(blocks):
            got = jnp.dot(hidden, ed[:, k * cols : (k + 1) * cols], preferred_element_type=f32)
            results[s, k] = got.astype(bf16).reshape(peers, cap, cols)

    def give_back(s, k):
        for o in far_first:
            back_copy(s, k, (me + o) % peers, me).start()
        own_back(s, k).start()

    def combine(s, k):
        below = jnp.logical_and(s >= z, z > 0)
        above = jnp.logical_and(s <= z, z < layers - 1)
        over = jnp.where(s == z, layers, s)
        wait_bytes(back.at[s, k], b_recv.at[s, k])
        both = lax.dot_general(
            weigh[s], back[s, k].reshape(slots, cols), (((0,), (0,)), ((), ())),
            preferred_element_type=f32,
        )
        got = both[:tokens] + both[tokens:]

        @pl.when(below)
        def _():
            wait_bytes(landed.at[s, k], c_recv.at[s, k])

        @pl.when(above)
        def _():
            wait_bytes(landed.at[over, k], c_recv.at[over, k])

        got = got + jnp.where(below, landed[s, k].astype(f32), 0.0)
        got = got + jnp.where(above, landed[over, k].astype(f32), 0.0)

        @pl.when(s == z)
        def _():
            lanes = pl.ds(pl.multiple_of(k * cols, cols), cols)
            out_ref[:, lanes] = (acc[k] + got).astype(bf16)

        @pl.when(s != z)
        def _():
            part[s, k] = got.astype(bf16)
            part_copy(s, k, jnp.where(s > z, 0, 1)).start()

    def shared():
        for load in loads[8:11]:
            load.wait()
        tall = jnp.concatenate([gathered[z, k] for k in range(blocks)], axis=1)
        hidden = mlp(tall, sg, su)
        for k in range(blocks):
            acc[k] = acc[k] + jnp.dot(
                hidden, sd[:, k * cols : (k + 1) * cols], preferred_element_type=f32
            )

    plans = [
        [code_of(step, layers, blocks) for step in steps_of(s, layers, blocks)]
        for s in range(layers)
    ]
    nothing = 3 * area + layers + 1
    base = 1 << nothing.bit_length()
    per_word = 30 // nothing.bit_length()
    count = -(-max(len(plan) for plan in plans) // per_word)
    words = []
    for i in range(count):
        word = jnp.int32(0)
        for s, plan in enumerate(plans):
            codes = plan[i * per_word : (i + 1) * per_word]
            codes = codes + [nothing] * (per_word - len(codes))
            packed_codes = sum(code * base**j for j, code in enumerate(codes))
            word = jnp.where(z == s, packed_codes, word)
        words.append(word)

    def act(code):
        number = code % area
        s = number // blocks
        k = number % blocks

        @pl.when(code < area)
        def _():
            arrive(s, k)

        @pl.when(code == 2 * blocks - 1)
        def _():
            for load in loads[11:]:
                load.wait()

        @pl.when(jnp.logical_and(code >= area, code < 2 * area))
        def _():
            give_back(s, k)

        @pl.when(jnp.logical_and(code >= 2 * area, code < 3 * area))
        def _():
            combine(s, k)

        @pl.when(jnp.logical_and(code >= 3 * area, code < 3 * area + layers))
        def _():
            expert(code - 3 * area)

        @pl.when(code == 3 * area + layers)
        def _():
            shared()

    def several(i, carry):
        word = words[0]
        for j in range(1, count):
            word = jnp.where(i == j, words[j], word)

        def single(j, word):
            act(word % base)
            return word // base

        lax.fori_loop(0, per_word, single, word)
        return carry

    lax.fori_loop(0, count, several, 0)

    def drain(s, carry):
        @pl.when(jnp.logical_and(s <= z, z < layers - 1))
        def _():
            wait_bytes(gathered.at[s], z_send.at[0, s])

        @pl.when(jnp.logical_and(s >= z, z > 0))
        def _():
            wait_bytes(gathered.at[s], z_send.at[1, s])

        wait_bytes(packed.at[s, :, pl.ds(1, peers - 1)], a_send.at[s])
        wait_bytes(results.at[s, :, pl.ds(1, peers - 1)], b_send.at[s])

        @pl.when(s != z)
        def _():
            wait_bytes(part.at[s], c_send.at[s])

        return carry

    lax.fori_loop(0, layers, drain, 0)
    for o in range(1, layers):
        meta_copy((z + o) % layers, z).wait_send()
    for o in range(1, cores):
        swap_copy((core + o) % cores, core).wait_send()

    @pl.when(gives_halo)
    def _():
        halo_copy(core).wait_send()

    @pl.when(gives_head)
    def _():
        head_copy(core).wait_send()


def on_device(
    residual,
    pool_input,
    group_maps,
    pool_scale,
    out_proj,
    norm_gain,
    shared_gate,
    shared_up,
    shared_down,
    expert_gate,
    expert_up,
    expert_down,
    expert_ids,
    route_score,
):
    rows, channels = pool_input.shape
    group_width = group_maps.shape[1]
    tokens, top = expert_ids.shape
    width = residual.shape[1]
    size_sp = lax.axis_size("sp")
    cores = lax.axis_size("tp")
    experts = size_sp * cores
    capacity = 3 * tokens * top // (2 * experts)
    cap = -(-capacity // 8) * 8
    layers = layer_count(size_sp)
    peers = experts // layers
    slots = peers * cap
    hidden_width = shared_gate.shape[1]
    expert_width = expert_gate.shape[2]
    cols = min(width, 512)
    blocks = width // cols
    bf16, f32 = jnp.bfloat16, jnp.float32
    dma = pltpu.SemaphoreType.DMA
    routed = (layers, blocks, peers, cap, cols)
    chunks = (layers, blocks, tokens, cols)
    return pl.pallas_call(
        functools.partial(layer_kernel, layers, peers, cores, cap),
        out_shape=pltpu.VMEM((tokens, width), bf16),
        in_specs=[pl.BlockSpec(memory_space=pltpu.HBM)] * 14,
        out_specs=pl.BlockSpec(memory_space=pltpu.VMEM),
        scratch_shapes=[
            pltpu.VMEM((tokens, width), bf16),
            pltpu.VMEM((rows, channels), bf16),
            pltpu.VMEM((cores, halo_rows, channels), bf16),
            pltpu.VMEM((cores, halo_rows, channels), bf16),
            pltpu.VMEM(group_maps.shape, bf16),
            pltpu.VMEM((group_maps.shape[0], 1, group_width), f32),
            pltpu.VMEM((1, width), f32),
            pltpu.VMEM((top, tokens), jnp.int32),
            pltpu.VMEM((top, tokens), f32),
            pltpu.VMEM((cores, rows // cores, channels), bf16),
            pltpu.VMEM((cores, rows // cores, channels), bf16),
            pltpu.VMEM(out_proj.shape, bf16),
            pltpu.VMEM(chunks, bf16),
            pltpu.VMEM((layers, 2 * top, tokens), f32),
            pltpu.VMEM((layers, slots, tokens), bf16),
            pltpu.VMEM((layers, slots, 2 * tokens), bf16),
            pltpu.VMEM(routed, bf16),
            pltpu.VMEM(routed, bf16),
            pltpu.VMEM(routed, bf16),
            pltpu.VMEM(routed, bf16),
            pltpu.VMEM(chunks, bf16),
            pltpu.VMEM((layers + 1, blocks, tokens, cols), bf16),
            pltpu.VMEM((blocks, tokens, cols), f32),
            pltpu.VMEM((width, hidden_width), bf16),
            pltpu.VMEM((width, hidden_width), bf16),
            pltpu.VMEM((hidden_width, width), bf16),
            pltpu.VMEM((width, expert_width), bf16),
            pltpu.VMEM((width, expert_width), bf16),
            pltpu.VMEM((expert_width, width), bf16),
            dma((14,)),
            dma((2,)),
            dma((2, cores)),
            dma((cores,)),
            dma((cores,)),
            dma((2, layers)),
            dma((layers, blocks)),
            dma((layers,)),
            dma((layers,)),
            dma((layers,)),
            dma((layers,)),
            dma((layers,)),
            dma((layers, blocks)),
            dma((layers,)),
            dma((layers + 1, blocks)),
        ],
        compiler_params=pltpu.CompilerParams(
            collective_id=0, has_side_effects=True, vmem_limit_bytes=56 * 1024 * 1024
        ),
    )(
        residual,
        pool_input,
        group_maps,
        pool_scale.reshape(-1, 1, group_width),
        out_proj,
        norm_gain.reshape(1, -1),
        shared_gate,
        shared_up,
        shared_down,
        expert_gate,
        expert_up,
        expert_down,
        expert_ids.T,
        route_score.T,
    )


def solution(mesh):
    in_specs = (
        P(("sp", "tp"), None),
        P("sp", "tp"),
        P(),
        P(),
        P(),
        P(),
        P(),
        P(),
        P(),
        P(("sp", "tp"), None, None),
        P(("sp", "tp"), None, None),
        P(("sp", "tp"), None, None),
        P(("sp", "tp"), None),
        P(("sp", "tp"), None),
    )
    out_specs = P(("sp", "tp"), None)
    return jax.shard_map(
        on_device, mesh=mesh, in_specs=in_specs, out_specs=out_specs, check_vma=False
    )
```

```python
import functools
import math

import jax
import jax.numpy as jnp
from jax import lax
from jax.experimental import pallas as pl
from jax.experimental.pallas import tpu as pltpu
from jax.sharding import PartitionSpec as P

windows = (2, 4, 8, 16)
epsilon = 1e-06
routed_scale = 2.5
halo_rows = 16


def layer_count(size_sp):
    return max(d for d in range(1, math.isqrt(size_sp) + 1) if size_sp % d == 0)


END = " ".join(
    (
        "a00 a01 a02 a03",
        "a10 a11 a12 a13",
        "a20 a21 a22 a23",
        "e1 b10 a30 a31",
        "b11 e2 c10 b20",
        "a32 e0 a33 c11",
        "c20 b21 b22 e3",
        "b30 b31 b32 b33",
        "c21 b23 b00 c30",
        "b01 c31 s c32",
        "c33 c22 b02 c23",
        "b12 b13 b03 c00",
        "c12 c01 c13 c02",
        "c03",
    )
)
MIDDLE = " ".join(
    (
        "a00 a01 a02 a03",
        "a10 a11 a12 a13",
        "a20 e1 a21 s",
        "e2 b20 a22 b10",
        "e0 a23 b00 e3",
        "b21 b30 b31 b01",
        "c20 c21 b32 b02",
        "b11 c30 b33 c31",
        "c00 b22 c32 b03",
        "b23 c10 c01 c33",
        "b12 c02 c22 b13",
        "c03 c11 c23 c12",
        "c13",
    )
)


def steps_of(z, layers, blocks):
    last = layers - 1
    if (layers, blocks) == (4, 4):
        steps = []
        for word in (END if z in (0, last) else MIDDLE).split():
            numbers = [int(digit) for digit in word[1:]]
            if word[0] in "ebc" and 2 * z > last:
                numbers[0] = last - numbers[0]
            steps.append((word[0], *numbers))
        return steps
    at = lambda r: sorted({s for s in (z - r, z + r) if 0 <= s < layers})
    reach = max(z, last - z)
    span = range(blocks)
    steps = [("a", 0, k) for k in span] + [("s",)]
    for r in range(1, reach + 2):
        if r <= reach:
            steps += [("a", r, k) for k in span]
        for s in at(r - 1):
            steps += [("e", s)] + [("b", s, k) for k in span]
    for r in range(reach, -1, -1):
        steps += [("c", s, k) for s in at(r) for k in span]
    return steps


def code_of(step, layers, blocks):
    area = layers * blocks
    base = {"a": 0, "b": area, "c": 2 * area, "e": 3 * area, "s": 3 * area + layers}[step[0]]
    if len(step) == 3:
        return base + step[1] * blocks + step[2]
    return base + sum(step[1:])


def layer_kernel(
    layers,
    peers,
    cores,
    cap,
    residual_hbm,
    pool_hbm,
    maps_hbm,
    scale_hbm,
    proj_hbm,
    gain_hbm,
    sg_hbm,
    su_hbm,
    sd_hbm,
    eg_hbm,
    eu_hbm,
    ed_hbm,
    ids_hbm,
    score_hbm,
    out_ref,
    residual,
    pool,
    halo,
    head,
    maps,
    scale,
    gain,
    ids,
    score,
    mixed,
    swapped,
    proj,
    gathered,
    metas,
    tables,
    weigh,
    packed,
    arrived,
    results,
    back,
    part,
    landed,
    acc,
    sg,
    su,
    sd,
    eg,
    eu,
    ed,
    w_sem,
    h_send,
    h_recv,
    x_send,
    x_recv,
    z_send,
    z_recv,
    m_send,
    m_recv,
    a_send,
    a_recv,
    b_send,
    b_recv,
    c_send,
    c_recv,
):
    per_layer = peers // cores
    sp = lax.axis_index("sp")
    size_sp = layers * per_layer
    core = lax.axis_index("tp")
    z = sp // per_layer
    q = sp % per_layer
    me = q * cores + core
    blocks, tokens, cols = acc.shape
    width = blocks * cols
    slots = peers * cap
    top = ids.shape[0]
    rows, channels = pool.shape
    group_width = maps.shape[1]
    groups_here = channels // group_width
    area = layers * blocks
    f32, bf16 = jnp.float32, jnp.bfloat16

    def in_column(s):
        return (s * per_layer + q, core)

    def in_layer(p):
        return (z * per_layer + p // cores, p % cores)

    def remote(src, dst, send, recv, to):
        return pltpu.make_async_remote_copy(
            src_ref=src,
            dst_ref=dst,
            send_sem=send,
            recv_sem=recv,
            device_id=to,
            device_id_type=pl.DeviceIdType.MESH,
        )

    def tell(to):
        pl.semaphore_signal(
            pltpu.get_barrier_semaphore(), inc=1, device_id=to,
            device_id_type=pl.DeviceIdType.MESH,
        )

    pairs = (
        (pool_hbm, pool),
        (ids_hbm, ids),
        (score_hbm, score),
        (maps_hbm, maps),
        (scale_hbm, scale),
        (proj_hbm, proj),
        (residual_hbm, residual),
        (gain_hbm, gain),
        (sg_hbm, sg),
        (su_hbm, su),
        (sd_hbm, sd),
        (eg_hbm.at[0], eg),
        (eu_hbm.at[0], eu),
        (ed_hbm.at[0], ed),
    )
    loads = [pltpu.make_async_copy(a, b, w_sem.at[i]) for i, (a, b) in enumerate(pairs)]
    for load in loads[:5]:
        load.start()
    for o in range(1, layers):
        tell(in_column((z + o) % layers))
    for o in range(1, peers):
        tell(in_layer((me + o) % peers))

    takes_halo = jnp.logical_and(sp > 0, core == 0)
    gives_halo = sp < size_sp - 1

    @pl.when(takes_halo)
    def _():
        for c in range(cores):
            tell((sp - 1, c))

    for load in loads[5:8]:
        load.start()

    loads[1].wait()
    loads[2].wait()
    experts = layers * peers
    ids_now = ids[...]
    score_now = score[...]
    expert_at = lax.broadcasted_iota(jnp.int32, (experts, tokens), 0)
    named = [(ids_now[k : k + 1] == expert_at).astype(f32) for k in range(top)]
    named_any = functools.reduce(jnp.add, named).astype(bf16)
    earlier = (
        lax.broadcasted_iota(jnp.int32, (tokens, tokens), 0)
        < lax.broadcasted_iota(jnp.int32, (tokens, tokens), 1)
    ).astype(bf16)
    rank = jnp.dot(named_any, earlier, preferred_element_type=f32)
    shares = score_now / jnp.sum(score_now, axis=0, keepdims=True) * routed_scale
    slot = [
        ids_now[k : k + 1].astype(f32) * cap + jnp.sum(rank * named[k], axis=0, keepdims=True)
        for k in range(top)
    ]
    metas[z] = jnp.concatenate(slot + [shares], axis=0)

    half = rows // cores

    def mix(before, own, start, c):
        place = start + lax.broadcasted_iota(jnp.int32, (own.shape[0], group_width), 0)
        out = []
        for g in range(groups_here):
            lanes = slice(g * group_width, (g + 1) * group_width)
            here = own[:, lanes]
            total = jnp.concatenate([before[:, lanes], here], axis=0)
            span = 1
            while span < windows[g % 4]:
                total = total + pltpu.roll(total, span, 0)
                span = span * 2
            divisor = jnp.minimum(place + 1, span).astype(f32)
            contrast = (total[halo_rows:] / divisor - here).astype(bf16)
            group = c * groups_here + g
            mapped = jnp.dot(contrast, maps[group], preferred_element_type=f32)
            out.append((mapped * scale[group]).astype(bf16))
        return jnp.concatenate(out, axis=1)

    for i in (0, 3, 4):
        loads[i].wait()
    for c in range(cores):
        start = c * half
        before = pool[max(start - halo_rows, 0) : max(start, halo_rows)].astype(f32)
        if c == 0:
            before = jnp.zeros_like(before)
        mixed[c] = mix(before, pool[start : start + half].astype(f32), sp * rows + start, core)

    pl.semaphore_wait(
        pltpu.get_barrier_semaphore(),
        layers - 1 + peers - 1 + jnp.where(gives_halo, 1, 0),
    )

    def halo_copy(source):
        return remote(
            pool.at[pl.ds(rows - halo_rows, halo_rows)], halo.at[source], h_send.at[0],
            h_recv.at[0, source], (jnp.minimum(sp + 1, size_sp - 1), 0),
        )

    def head_copy(source):
        return remote(
            pool.at[pl.ds(0, halo_rows)], head.at[source], h_send.at[1],
            h_recv.at[1, source], (sp, 0),
        )

    def swap_copy(p, source):
        return remote(
            mixed.at[p], swapped.at[source], x_send.at[p], x_recv.at[source], (sp, p)
        )

    @pl.when(gives_halo)
    def _():
        halo_copy(core).start()

    for o in range(1, cores):
        swap_copy((core + o) % cores, core).start()

    gives_head = jnp.logical_and(sp > 0, core > 0)

    @pl.when(gives_head)
    def _():
        head_copy(core).start()

    def meta_copy(target, source):
        return remote(
            metas.at[source], metas.at[source], m_send.at[target], m_recv.at[source],
            in_column(target),
        )

    for o in range(1, layers):
        meta_copy((z + o) % layers, z).start()
    for load in loads[8:11]:
        load.start()

    def neighbour(side):
        return in_column(jnp.clip(jnp.where(side == 0, z + 1, z - 1), 0, layers - 1))

    def chunk_copy(s, k, side):
        return remote(
            gathered.at[s, k], gathered.at[s, k], z_send.at[side, s], z_recv.at[s, k],
            neighbour(side),
        )

    def pack_copy(s, k, p, source):
        return remote(
            packed.at[s, k, p], arrived.at[s, k, source], a_send.at[s],
            a_recv.at[s], in_layer(p),
        )

    def back_copy(s, k, p, source):
        return remote(
            results.at[s, k, p], back.at[s, k, source], b_send.at[s],
            b_recv.at[s, k], in_layer(p),
        )

    def own_pack(s, k):
        return pltpu.make_async_copy(
            packed.at[s, k, me], arrived.at[s, k, me], a_recv.at[s]
        )

    def own_back(s, k):
        return pltpu.make_async_copy(
            results.at[s, k, me], back.at[s, k, me], b_recv.at[s, k]
        )

    def part_copy(s, k, side):
        slot = jnp.where(jnp.logical_and(side == 1, s == z - 1), layers, s)
        return remote(
            part.at[s, k], landed.at[slot, k], c_send.at[s], c_recv.at[slot, k],
            neighbour(side),
        )

    def wait_bytes(ref, sem):
        pltpu.make_async_copy(ref, ref, sem).wait()

    far_first = sorted(range(1, peers), key=lambda o: (o % cores, -o % 3, o))

    for load in loads[11:]:
        load.start()
    for o in range(1, cores):
        p = (core + o) % cores
        swap_copy(p, p).wait_recv()

    @pl.when(takes_halo)
    def _():
        for c in range(cores):
            halo_copy(c).wait_recv()
            own = pool[:halo_rows]
            if c > 0:
                head_copy(c).wait_recv()
                own = head[c]
            fixed = mix(halo[c].astype(f32), own.astype(f32), sp * rows, c)
            if c == 0:
                mixed[0, :halo_rows] = fixed
            else:
                swapped[c, :halo_rows] = fixed

    for load in loads[5:8]:
        load.wait()

    def channels_of(c):
        return pl.ds(pl.multiple_of(c * channels, channels), channels)

    for k in range(blocks):
        lanes = slice(k * cols, (k + 1) * cols)
        total = residual[:, lanes].astype(f32) + jnp.dot(
            mixed[core], proj[channels_of(core), lanes], preferred_element_type=f32
        )
        for o in range(1, cores):
            p = (core + o) % cores
            total = total + jnp.dot(
                swapped[p], proj[channels_of(p), lanes], preferred_element_type=f32
            )
        acc[k] = total
    squares = jnp.zeros((tokens, 1), f32)
    for k in range(blocks):
        settled = acc[k].astype(bf16).astype(f32)
        acc[k] = settled
        squares = squares + jnp.sum(settled * settled, axis=1, keepdims=True)
    inverse = lax.rsqrt(squares / width + epsilon)
    for k in range(blocks):
        gathered[z, k] = (acc[k] * inverse * gain[:, k * cols : (k + 1) * cols]).astype(bf16)

        @pl.when(z < layers - 1)
        def _():
            chunk_copy(z, k, 0).start()

        @pl.when(z > 0)
        def _():
            chunk_copy(z, k, 1).start()

    def prepare(s):
        rows_now = metas[s]
        ids_down = lax.broadcasted_iota(jnp.int32, (slots, tokens), 0).astype(f32)
        ids_down = ids_down + (z * slots).astype(f32)
        table = jnp.zeros((slots, tokens), f32)
        value = jnp.zeros((slots, tokens), f32)
        for k in range(top):
            hit = ids_down == rows_now[k : k + 1]
            table = jnp.where(hit, 1.0, table)
            value = jnp.where(hit, rows_now[top + k : top + k + 1], value)
        tables[s] = table.astype(bf16)
        high = value.astype(bf16)
        weigh[s, :, :tokens] = high
        weigh[s, :, tokens:] = (value - high.astype(f32)).astype(bf16)

    def arrive(r, k):
        def one(side, carry):
            s = jnp.where(side == 0, z - r, z + r)
            here = jnp.logical_and(s >= 0, s < layers)
            here = jnp.logical_and(here, jnp.logical_or(r > 0, side == 0))
            far = jnp.logical_and(here, r > 0)
            onward = jnp.logical_and(far, jnp.where(side == 0, z < layers - 1, z > 0))
            s = jnp.clip(s, 0, layers - 1)

            @pl.when(far)
            def _():
                chunk_copy(s, k, 0).wait_recv()

            @pl.when(onward)
            def _():
                chunk_copy(s, k, side).start()

            @pl.when(jnp.logical_and(far, k == 0))
            def _():
                meta_copy(z, s).wait_recv()

            @pl.when(jnp.logical_and(here, k == 0))
            def _():
                prepare(s)

            @pl.when(here)
            def _():
                got = jnp.dot(tables[s], gathered[s, k], preferred_element_type=f32)
                packed[s, k] = got.astype(bf16).reshape(peers, cap, cols)
                for o in far_first:
                    pack_copy(s, k, (me + o) % peers, me).start()
                own_pack(s, k).start()

            return carry

        lax.fori_loop(0, 2, one, 0)

    def mlp(tall, w_gate, w_up):
        gate = jnp.dot(tall, w_gate[...], preferred_element_type=f32)
        up = jnp.dot(tall, w_up[...], preferred_element_type=f32)
        return (gate / (1.0 + jnp.exp(-gate)) * up).astype(bf16)

    def expert(s):
        wait_bytes(arrived.at[s], a_recv.at[s])
        tall = jnp.concatenate(
            [arrived[s, k].reshape(slots, cols) for k in range(blocks)], axis=1
        )
        hidden = mlp(tall, eg, eu)
        for k in range(blocks):
            got = jnp.dot(hidden, ed[:, k * cols : (k + 1) * cols], preferred_element_type=f32)
            results[s, k] = got.astype(bf16).reshape(peers, cap, cols)

    def give_back(s, k):
        for o in far_first:
            back_copy(s, k, (me + o) % peers, me).start()
        own_back(s, k).start()

    def combine(s, k):
        below = jnp.logical_and(s >= z, z > 0)
        above = jnp.logical_and(s <= z, z < layers - 1)
        over = jnp.where(s == z, layers, s)
        wait_bytes(back.at[s, k], b_recv.at[s, k])
        both = lax.dot_general(
            weigh[s], back[s, k].reshape(slots, cols), (((0,), (0,)), ((), ())),
            preferred_element_type=f32,
        )
        got = both[:tokens] + both[tokens:]

        @pl.when(below)
        def _():
            wait_bytes(landed.at[s, k], c_recv.at[s, k])

        @pl.when(above)
        def _():
            wait_bytes(landed.at[over, k], c_recv.at[over, k])

        got = got + jnp.where(below, landed[s, k].astype(f32), 0.0)
        got = got + jnp.where(above, landed[over, k].astype(f32), 0.0)

        @pl.when(s == z)
        def _():
            lanes = pl.ds(pl.multiple_of(k * cols, cols), cols)
            out_ref[:, lanes] = (acc[k] + got).astype(bf16)

        @pl.when(s != z)
        def _():
            part[s, k] = got.astype(bf16)
            part_copy(s, k, jnp.where(s > z, 0, 1)).start()

    def shared():
        for load in loads[8:11]:
            load.wait()
        tall = jnp.concatenate([gathered[z, k] for k in range(blocks)], axis=1)
        hidden = mlp(tall, sg, su)
        for k in range(blocks):
            acc[k] = acc[k] + jnp.dot(
                hidden, sd[:, k * cols : (k + 1) * cols], preferred_element_type=f32
            )

    plans = [
        [code_of(step, layers, blocks) for step in steps_of(s, layers, blocks)]
        for s in range(layers)
    ]
    nothing = 3 * area + layers + 1
    base = 1 << nothing.bit_length()
    per_word = 30 // nothing.bit_length()
    count = -(-max(len(plan) for plan in plans) // per_word)
    words = []
    for i in range(count):
        word = jnp.int32(0)
        for s, plan in enumerate(plans):
            codes = plan[i * per_word : (i + 1) * per_word]
            codes = codes + [nothing] * (per_word - len(codes))
            packed_codes = sum(code * base**j for j, code in enumerate(codes))
            word = jnp.where(z == s, packed_codes, word)
        words.append(word)

    def act(code):
        number = code % area
        s = number // blocks
        k = number % blocks

        @pl.when(code < area)
        def _():
            arrive(s, k)

        @pl.when(code == 2 * blocks - 1)
        def _():
            for load in loads[11:]:
                load.wait()

        @pl.when(jnp.logical_and(code >= area, code < 2 * area))
        def _():
            give_back(s, k)

        @pl.when(jnp.logical_and(code >= 2 * area, code < 3 * area))
        def _():
            combine(s, k)

        @pl.when(jnp.logical_and(code >= 3 * area, code < 3 * area + layers))
        def _():
            expert(code - 3 * area)

        @pl.when(code == 3 * area + layers)
        def _():
            shared()

    def several(i, carry):
        word = words[0]
        for j in range(1, count):
            word = jnp.where(i == j, words[j], word)

        def single(j, word):
            act(word % base)
            return word // base

        lax.fori_loop(0, per_word, single, word)
        return carry

    lax.fori_loop(0, count, several, 0)

    def drain(s, carry):
        @pl.when(jnp.logical_and(s <= z, z < layers - 1))
        def _():
            wait_bytes(gathered.at[s], z_send.at[0, s])

        @pl.when(jnp.logical_and(s >= z, z > 0))
        def _():
            wait_bytes(gathered.at[s], z_send.at[1, s])

        wait_bytes(packed.at[s, :, pl.ds(1, peers - 1)], a_send.at[s])
        wait_bytes(results.at[s, :, pl.ds(1, peers - 1)], b_send.at[s])

        @pl.when(s != z)
        def _():
            wait_bytes(part.at[s], c_send.at[s])

        return carry

    lax.fori_loop(0, layers, drain, 0)
    for o in range(1, layers):
        meta_copy((z + o) % layers, z).wait_send()
    for o in range(1, cores):
        swap_copy((core + o) % cores, core).wait_send()

    @pl.when(gives_halo)
    def _():
        halo_copy(core).wait_send()

    @pl.when(gives_head)
    def _():
        head_copy(core).wait_send()


def on_device(
    residual,
    pool_input,
    group_maps,
    pool_scale,
    out_proj,
    norm_gain,
    shared_gate,
    shared_up,
    shared_down,
    expert_gate,
    expert_up,
    expert_down,
    expert_ids,
    route_score,
):
    rows, channels = pool_input.shape
    group_width = group_maps.shape[1]
    tokens, top = expert_ids.shape
    width = residual.shape[1]
    size_sp = lax.axis_size("sp")
    cores = lax.axis_size("tp")
    experts = size_sp * cores
    capacity = 3 * tokens * top // (2 * experts)
    cap = -(-capacity // 8) * 8
    layers = layer_count(size_sp)
    peers = experts // layers
    slots = peers * cap
    hidden_width = shared_gate.shape[1]
    expert_width = expert_gate.shape[2]
    cols = min(width, 512)
    blocks = width // cols
    bf16, f32 = jnp.bfloat16, jnp.float32
    dma = pltpu.SemaphoreType.DMA
    routed = (layers, blocks, peers, cap, cols)
    chunks = (layers, blocks, tokens, cols)
    return pl.pallas_call(
        functools.partial(layer_kernel, layers, peers, cores, cap),
        out_shape=pltpu.VMEM((tokens, width), bf16),
        in_specs=[pl.BlockSpec(memory_space=pltpu.HBM)] * 14,
        out_specs=pl.BlockSpec(memory_space=pltpu.VMEM),
        scratch_shapes=[
            pltpu.VMEM((tokens, width), bf16),
            pltpu.VMEM((rows, channels), bf16),
            pltpu.VMEM((cores, halo_rows, channels), bf16),
            pltpu.VMEM((cores, halo_rows, channels), bf16),
            pltpu.VMEM(group_maps.shape, bf16),
            pltpu.VMEM((group_maps.shape[0], 1, group_width), f32),
            pltpu.VMEM((1, width), f32),
            pltpu.VMEM((top, tokens), jnp.int32),
            pltpu.VMEM((top, tokens), f32),
            pltpu.VMEM((cores, rows // cores, channels), bf16),
            pltpu.VMEM((cores, rows // cores, channels), bf16),
            pltpu.VMEM(out_proj.shape, bf16),
            pltpu.VMEM(chunks, bf16),
            pltpu.VMEM((layers, 2 * top, tokens), f32),
            pltpu.VMEM((layers, slots, tokens), bf16),
            pltpu.VMEM((layers, slots, 2 * tokens), bf16),
            pltpu.VMEM(routed, bf16),
            pltpu.VMEM(routed, bf16),
            pltpu.VMEM(routed, bf16),
            pltpu.VMEM(routed, bf16),
            pltpu.VMEM(chunks, bf16),
            pltpu.VMEM((layers + 1, blocks, tokens, cols), bf16),
            pltpu.VMEM((blocks, tokens, cols), f32),
            pltpu.VMEM((width, hidden_width), bf16),
            pltpu.VMEM((width, hidden_width), bf16),
            pltpu.VMEM((hidden_width, width), bf16),
            pltpu.VMEM((width, expert_width), bf16),
            pltpu.VMEM((width, expert_width), bf16),
            pltpu.VMEM((expert_width, width), bf16),
            dma((14,)),
            dma((2,)),
            dma((2, cores)),
            dma((cores,)),
            dma((cores,)),
            dma((2, layers)),
            dma((layers, blocks)),
            dma((layers,)),
            dma((layers,)),
            dma((layers,)),
            dma((layers,)),
            dma((layers,)),
            dma((layers, blocks)),
            dma((layers,)),
            dma((layers + 1, blocks)),
        ],
        compiler_params=pltpu.CompilerParams(
            collective_id=0, has_side_effects=True, vmem_limit_bytes=56 * 1024 * 1024
        ),
    )(
        residual,
        pool_input,
        group_maps,
        pool_scale.reshape(-1, 1, group_width),
        out_proj,
        norm_gain.reshape(1, -1),
        shared_gate,
        shared_up,
        shared_down,
        expert_gate,
        expert_up,
        expert_down,
        expert_ids.T,
        route_score.T,
    )


def solution(mesh):
    in_specs = (
        P(("sp", "tp"), None),
        P("sp", "tp"),
        P(),
        P(),
        P(),
        P(),
        P(),
        P(),
        P(),
        P(("sp", "tp"), None, None),
        P(("sp", "tp"), None, None),
        P(("sp", "tp"), None, None),
        P(("sp", "tp"), None),
        P(("sp", "tp"), None),
    )
    out_specs = P(("sp", "tp"), None)
    return jax.shard_map(
        on_device, mesh=mesh, in_specs=in_specs, out_specs=out_specs, check_vma=False
    )
```

```python
import functools
import math

import jax
import jax.numpy as jnp
from jax import lax
from jax.experimental import pallas as pl
from jax.experimental.pallas import tpu as pltpu
from jax.sharding import PartitionSpec as P

windows = (2, 4, 8, 16)
epsilon = 1e-06
routed_scale = 2.5
halo_rows = 16


def layer_count(size_sp):
    return max(d for d in range(1, math.isqrt(size_sp) + 1) if size_sp % d == 0)


END = (
    " ".join(
        (
            "a00 a01 a02 a03",
            "s a10 a11 a12",
            "a13 a20 a21 a22",
            "a23 e1 b10 a30",
            "a31 a32 e2 b20",
            "a33 c20 c10 b21",
            "e3 b30 b31 b22",
            "b32 c21 b33 b11",
            "c30 b12 e0 c31",
            "c32 b23 c33 b00",
            "c22 b13 c00 b01",
            "b02 b03 c23 c11",
            "c12 c01 c13 c02",
            "c03",
        )
    ),
    " ".join(
        (
            "a00 a01 a02 a03",
            "a10 a11 a12 a13",
            "a20 a21 a22 a23",
            "e0 e1 b10 e2",
            "a30 b20 a31 a32",
            "c10 a33 b21 c20",
            "b00 e3 b30 c21",
            "b31 c30 b32 c31",
            "b33 b11 c32 b22",
            "b23 b12 c11 c33",
            "b01 b13 b02 c22",
            "c23 s c00 c12",
            "b03 c13 c01 c02",
            "c03",
        )
    ),
)
MIDDLE = (
    " ".join(
        (
            "a00 a01 a02 a03",
            "a10 a11 a12 a13",
            "a20 e1 b10 a21",
            "a22 a23 e2 e0",
            "b20 b21 e3 b00",
            "b30 c20 b31 b01",
            "b02 c21 b32 b11",
            "b33 c30 c31 c00",
            "b03 s c32 b22",
            "c01 b23 c10 b12",
            "c33 c02 c03 b13",
            "c22 c23 c11 c12",
            "c13",
        )
    ),
    " ".join(
        (
            "a00 a01 a02 a03",
            "a10 a11 a12 s",
            "a13 e1 e2 b20",
            "a20 a21 a22 a23",
            "b10 e0 b00 b21",
            "e3 b30 c20 b31",
            "b22 b01 b02 c21",
            "b32 b33 c30 b03",
            "c31 c32 c00 c01",
            "c02 b23 c33 b11",
            "b12 c22 c10 c23",
            "c03 b13 c11 c12",
            "c13",
        )
    ),
)


def steps_of(z, core, layers, blocks):
    last = layers - 1
    if (layers, blocks) == (4, 4) and core < len(END):
        steps = []
        for word in (END if z in (0, last) else MIDDLE)[core].split():
            numbers = [int(digit) for digit in word[1:]]
            if word[0] in "ebc" and 2 * z > last:
                numbers[0] = last - numbers[0]
            steps.append((word[0], *numbers))
        return steps
    at = lambda r: sorted({s for s in (z - r, z + r) if 0 <= s < layers})
    reach = max(z, last - z)
    span = range(blocks)
    steps = [("a", 0, k) for k in span] + [("s",)]
    for r in range(1, reach + 2):
        if r <= reach:
            steps += [("a", r, k) for k in span]
        for s in at(r - 1):
            steps += [("e", s)] + [("b", s, k) for k in span]
    for r in range(reach, -1, -1):
        steps += [("c", s, k) for s in at(r) for k in span]
    return steps


def code_of(step, layers, blocks):
    area = layers * blocks
    base = {"a": 0, "b": area, "c": 2 * area, "e": 3 * area, "s": 3 * area + layers}[step[0]]
    if len(step) == 3:
        return base + step[1] * blocks + step[2]
    return base + sum(step[1:])


def layer_kernel(
    layers,
    peers,
    cores,
    cap,
    residual_hbm,
    pool_hbm,
    maps_hbm,
    scale_hbm,
    proj_hbm,
    gain_hbm,
    sg_hbm,
    su_hbm,
    sd_hbm,
    eg_hbm,
    eu_hbm,
    ed_hbm,
    ids_hbm,
    score_hbm,
    out_ref,
    residual,
    pool,
    halo,
    head,
    maps,
    scale,
    gain,
    ids,
    score,
    mixed,
    swapped,
    proj,
    gathered,
    metas,
    tables,
    weigh,
    packed,
    arrived,
    results,
    back,
    part,
    landed,
    acc,
    hidden,
    sg,
    su,
    sd,
    eg,
    eu,
    ed,
    w_sem,
    h_send,
    h_recv,
    x_send,
    x_recv,
    z_send,
    z_recv,
    m_send,
    m_recv,
    a_send,
    a_recv,
    b_send,
    b_recv,
    c_send,
    c_recv,
):
    per_layer = peers // cores
    sp = lax.axis_index("sp")
    size_sp = layers * per_layer
    core = lax.axis_index("tp")
    z = sp // per_layer
    q = sp % per_layer
    me = q * cores + core
    blocks, tokens, cols = acc.shape
    width = blocks * cols
    slots = peers * cap
    top = ids.shape[0]
    rows, channels = pool.shape
    group_width = maps.shape[1]
    groups_here = channels // group_width
    area = layers * blocks
    f32, bf16 = jnp.float32, jnp.bfloat16

    def in_column(s):
        return (s * per_layer + q, core)

    def in_layer(p):
        return (z * per_layer + p // cores, p % cores)

    def remote(src, dst, send, recv, to):
        return pltpu.make_async_remote_copy(
            src_ref=src,
            dst_ref=dst,
            send_sem=send,
            recv_sem=recv,
            device_id=to,
            device_id_type=pl.DeviceIdType.MESH,
        )

    def tell(to):
        pl.semaphore_signal(
            pltpu.get_barrier_semaphore(), inc=1, device_id=to,
            device_id_type=pl.DeviceIdType.MESH,
        )

    pairs = (
        (pool_hbm, pool),
        (ids_hbm, ids),
        (score_hbm, score),
        (maps_hbm, maps),
        (scale_hbm, scale),
        (proj_hbm, proj),
        (residual_hbm, residual),
        (gain_hbm, gain),
        (sg_hbm, sg),
        (su_hbm, su),
        (sd_hbm, sd),
        (eg_hbm.at[0], eg),
        (eu_hbm.at[0], eu),
        (ed_hbm.at[0], ed),
    )
    loads = [pltpu.make_async_copy(a, b, w_sem.at[i]) for i, (a, b) in enumerate(pairs)]
    for load in loads[:5]:
        load.start()
    for o in range(1, layers):
        tell(in_column((z + o) % layers))
    for o in range(1, peers):
        tell(in_layer((me + o) % peers))

    takes_halo = jnp.logical_and(sp > 0, core == 0)
    gives_halo = sp < size_sp - 1

    @pl.when(takes_halo)
    def _():
        for c in range(cores):
            tell((sp - 1, c))

    for load in loads[5:8]:
        load.start()

    half = rows // cores

    def mix(before, own, start, c):
        place = start + lax.broadcasted_iota(jnp.int32, (own.shape[0], group_width), 0)
        out = []
        for g in range(groups_here):
            lanes = slice(g * group_width, (g + 1) * group_width)
            here = own[:, lanes]
            total = jnp.concatenate([before[:, lanes], here], axis=0)
            span = 1
            while span < windows[g % 4]:
                total = total + pltpu.roll(total, span, 0)
                span = span * 2
            divisor = jnp.minimum(place + 1, span).astype(f32)
            contrast = (total[halo_rows:] / divisor - here).astype(bf16)
            group = c * groups_here + g
            mapped = jnp.dot(contrast, maps[group], preferred_element_type=f32)
            out.append((mapped * scale[group]).astype(bf16))
        return jnp.concatenate(out, axis=1)

    for i in (0, 3, 4):
        loads[i].wait()
    for c in range(cores):
        start = c * half
        before = pool[max(start - halo_rows, 0) : max(start, halo_rows)].astype(f32)
        if c == 0:
            before = jnp.zeros_like(before)
        mixed[c] = mix(before, pool[start : start + half].astype(f32), sp * rows + start, core)

    pl.semaphore_wait(
        pltpu.get_barrier_semaphore(),
        layers - 1 + peers - 1 + jnp.where(gives_halo, 1, 0),
    )

    def halo_copy(source):
        return remote(
            pool.at[pl.ds(rows - halo_rows, halo_rows)], halo.at[source], h_send.at[0],
            h_recv.at[0, source], (jnp.minimum(sp + 1, size_sp - 1), 0),
        )

    def head_copy(source):
        return remote(
            pool.at[pl.ds(0, halo_rows)], head.at[source], h_send.at[1],
            h_recv.at[1, source], (sp, 0),
        )

    def swap_copy(p, source):
        return remote(
            mixed.at[p], swapped.at[source], x_send.at[p], x_recv.at[source], (sp, p)
        )

    @pl.when(gives_halo)
    def _():
        halo_copy(core).start()

    for o in range(1, cores):
        swap_copy((core + o) % cores, core).start()

    gives_head = jnp.logical_and(sp > 0, core > 0)

    @pl.when(gives_head)
    def _():
        head_copy(core).start()

    def meta_copy(target, source):
        return remote(
            metas.at[source], metas.at[source], m_send.at[target], m_recv.at[source],
            in_column(target),
        )

    for load in loads[8:11]:
        load.start()

    def neighbour(side):
        return in_column(jnp.clip(jnp.where(side == 0, z + 1, z - 1), 0, layers - 1))

    def chunk_copy(s, k, side):
        return remote(
            gathered.at[s, k], gathered.at[s, k], z_send.at[side, s], z_recv.at[s, k],
            neighbour(side),
        )

    def pack_copy(s, k, p, source):
        return remote(
            packed.at[s, k, p], arrived.at[s, k, source], a_send.at[s],
            a_recv.at[s], in_layer(p),
        )

    def back_copy(s, k, p, source):
        return remote(
            results.at[s, k, p], back.at[s, k, source], b_send.at[s],
            b_recv.at[s, k], in_layer(p),
        )

    def own_pack(s, k):
        return pltpu.make_async_copy(
            packed.at[s, k, me], arrived.at[s, k, me], a_recv.at[s]
        )

    def own_back(s, k):
        return pltpu.make_async_copy(
            results.at[s, k, me], back.at[s, k, me], b_recv.at[s, k]
        )

    def part_copy(s, k, side):
        slot = jnp.where(jnp.logical_and(side == 1, s == z - 1), layers, s)
        return remote(
            part.at[s, k], landed.at[slot, k], c_send.at[s], c_recv.at[slot, k],
            neighbour(side),
        )

    def wait_bytes(ref, sem):
        pltpu.make_async_copy(ref, ref, sem).wait()

    far_first = sorted(range(1, peers), key=lambda o: (o % cores, -o % 3, o))

    for load in loads[11:]:
        load.start()
    loads[1].wait()
    loads[2].wait()
    experts = layers * peers
    ids_now = ids[...]
    score_now = score[...]
    expert_at = lax.broadcasted_iota(jnp.int32, (experts, tokens), 0)
    named = [(ids_now[k : k + 1] == expert_at).astype(f32) for k in range(top)]
    named_any = functools.reduce(jnp.add, named).astype(bf16)
    earlier = (
        lax.broadcasted_iota(jnp.int32, (tokens, tokens), 0)
        < lax.broadcasted_iota(jnp.int32, (tokens, tokens), 1)
    ).astype(bf16)
    rank = jnp.dot(named_any, earlier, preferred_element_type=f32)
    shares = score_now / jnp.sum(score_now, axis=0, keepdims=True) * routed_scale
    slot = [
        ids_now[k : k + 1].astype(f32) * cap + jnp.sum(rank * named[k], axis=0, keepdims=True)
        for k in range(top)
    ]
    metas[z] = jnp.concatenate(slot + [shares], axis=0)

    for o in range(1, layers):
        meta_copy((z + o) % layers, z).start()

    for o in range(1, cores):
        p = (core + o) % cores
        swap_copy(p, p).wait_recv()

    @pl.when(takes_halo)
    def _():
        for c in range(cores):
            halo_copy(c).wait_recv()
            own = pool[:halo_rows]
            if c > 0:
                head_copy(c).wait_recv()
                own = head[c]
            fixed = mix(halo[c].astype(f32), own.astype(f32), sp * rows, c)
            if c == 0:
                mixed[0, :halo_rows] = fixed
            else:
                swapped[c, :halo_rows] = fixed

    for load in loads[5:8]:
        load.wait()

    def channels_of(c):
        return pl.ds(pl.multiple_of(c * channels, channels), channels)

    for k in range(blocks):
        lanes = slice(k * cols, (k + 1) * cols)
        total = residual[:, lanes].astype(f32) + jnp.dot(
            mixed[core], proj[channels_of(core), lanes], preferred_element_type=f32
        )
        for o in range(1, cores):
            p = (core + o) % cores
            total = total + jnp.dot(
                swapped[p], proj[channels_of(p), lanes], preferred_element_type=f32
            )
        acc[k] = total
    squares = jnp.zeros((tokens, 1), f32)
    for k in range(blocks):
        settled = acc[k].astype(bf16).astype(f32)
        acc[k] = settled
        squares = squares + jnp.sum(settled * settled, axis=1, keepdims=True)
    inverse = lax.rsqrt(squares / width + epsilon)
    for k in range(blocks):
        gathered[z, k] = (acc[k] * inverse * gain[:, k * cols : (k + 1) * cols]).astype(bf16)

        @pl.when(z < layers - 1)
        def _():
            chunk_copy(z, k, 0).start()

        @pl.when(z > 0)
        def _():
            chunk_copy(z, k, 1).start()

    def prepare(s):
        rows_now = metas[s]
        ids_down = lax.broadcasted_iota(jnp.int32, (slots, tokens), 0).astype(f32)
        ids_down = ids_down + (z * slots).astype(f32)
        table = jnp.zeros((slots, tokens), f32)
        value = jnp.zeros((slots, tokens), f32)
        for k in range(top):
            hit = ids_down == rows_now[k : k + 1]
            table = jnp.where(hit, 1.0, table)
            value = jnp.where(hit, rows_now[top + k : top + k + 1], value)
        tables[s] = table.astype(bf16)
        high = value.astype(bf16)
        weigh[s, :, :tokens] = high
        weigh[s, :, tokens:] = (value - high.astype(f32)).astype(bf16)

    def arrive(r, k):
        def one(side, carry):
            s = jnp.where(side == 0, z - r, z + r)
            here = jnp.logical_and(s >= 0, s < layers)
            here = jnp.logical_and(here, jnp.logical_or(r > 0, side == 0))
            far = jnp.logical_and(here, r > 0)
            onward = jnp.logical_and(far, jnp.where(side == 0, z < layers - 1, z > 0))
            s = jnp.clip(s, 0, layers - 1)

            @pl.when(far)
            def _():
                chunk_copy(s, k, 0).wait_recv()

            @pl.when(onward)
            def _():
                chunk_copy(s, k, side).start()

            @pl.when(jnp.logical_and(far, k == 0))
            def _():
                meta_copy(z, s).wait_recv()

            @pl.when(jnp.logical_and(here, k == 0))
            def _():
                prepare(s)

            @pl.when(here)
            def _():
                got = jnp.dot(tables[s], gathered[s, k], preferred_element_type=f32)
                packed[s, k] = got.astype(bf16).reshape(peers, cap, cols)
                for o in far_first:
                    pack_copy(s, k, (me + o) % peers, me).start()
                own_pack(s, k).start()

            return carry

        lax.fori_loop(0, 2, one, 0)

    def mlp(tall, w_gate, w_up):
        gate = jnp.dot(tall, w_gate[...], preferred_element_type=f32)
        up = jnp.dot(tall, w_up[...], preferred_element_type=f32)
        return (gate / (1.0 + jnp.exp(-gate)) * up).astype(bf16)

    def expert(s):
        wait_bytes(arrived.at[s], a_recv.at[s])
        tall = jnp.concatenate(
            [arrived[s, k].reshape(slots, cols) for k in range(blocks)], axis=1
        )
        hidden[s] = mlp(tall, eg, eu)

    def give_back(s, k):
        lanes = pl.ds(pl.multiple_of(k * cols, cols), cols)
        got = jnp.dot(hidden[s], ed[:, lanes], preferred_element_type=f32)
        results[s, k] = got.astype(bf16).reshape(peers, cap, cols)
        for o in far_first:
            back_copy(s, k, (me + o) % peers, me).start()
        own_back(s, k).start()

    def combine(s, k):
        below = jnp.logical_and(s >= z, z > 0)
        above = jnp.logical_and(s <= z, z < layers - 1)
        over = jnp.where(s == z, layers, s)
        wait_bytes(back.at[s, k], b_recv.at[s, k])
        both = lax.dot_general(
            weigh[s], back[s, k].reshape(slots, cols), (((0,), (0,)), ((), ())),
            preferred_element_type=f32,
        )
        got = both[:tokens] + both[tokens:]

        @pl.when(below)
        def _():
            wait_bytes(landed.at[s, k], c_recv.at[s, k])

        @pl.when(above)
        def _():
            wait_bytes(landed.at[over, k], c_recv.at[over, k])

        got = got + jnp.where(below, landed[s, k].astype(f32), 0.0)
        got = got + jnp.where(above, landed[over, k].astype(f32), 0.0)

        @pl.when(s == z)
        def _():
            lanes = pl.ds(pl.multiple_of(k * cols, cols), cols)
            out_ref[:, lanes] = (acc[k] + got).astype(bf16)

        @pl.when(s != z)
        def _():
            part[s, k] = got.astype(bf16)
            part_copy(s, k, jnp.where(s > z, 0, 1)).start()

    def shared():
        for load in loads[8:11]:
            load.wait()
        tall = jnp.concatenate([gathered[z, k] for k in range(blocks)], axis=1)
        inner = mlp(tall, sg, su)
        for k in range(blocks):
            acc[k] = acc[k] + jnp.dot(
                inner, sd[:, k * cols : (k + 1) * cols], preferred_element_type=f32
            )

    plans = {
        (s, c): [code_of(step, layers, blocks) for step in steps_of(s, c, layers, blocks)]
        for s in range(layers)
        for c in range(cores)
    }
    nothing = 3 * area + layers + 1
    base = 1 << nothing.bit_length()
    per_word = 30 // nothing.bit_length()
    count = -(-max(len(plan) for plan in plans.values()) // per_word)
    words = []
    for i in range(count):
        word = jnp.int32(0)
        for (s, c), plan in plans.items():
            codes = plan[i * per_word : (i + 1) * per_word]
            codes = codes + [nothing] * (per_word - len(codes))
            packed_codes = sum(code * base**j for j, code in enumerate(codes))
            word = jnp.where(jnp.logical_and(z == s, core == c), packed_codes, word)
        words.append(word)

    def act(code):
        number = code % area
        s = number // blocks
        k = number % blocks

        @pl.when(code < area)
        def _():
            arrive(s, k)

        @pl.when(code == 2 * blocks - 1)
        def _():
            for load in loads[11:]:
                load.wait()

        @pl.when(jnp.logical_and(code >= area, code < 2 * area))
        def _():
            give_back(s, k)

        @pl.when(jnp.logical_and(code >= 2 * area, code < 3 * area))
        def _():
            combine(s, k)

        @pl.when(jnp.logical_and(code >= 3 * area, code < 3 * area + layers))
        def _():
            expert(code - 3 * area)

        @pl.when(code == 3 * area + layers)
        def _():
            shared()

    def several(i, carry):
        word = words[0]
        for j in range(1, count):
            word = jnp.where(i == j, words[j], word)

        def single(j, word):
            act(word % base)
            return word // base

        lax.fori_loop(0, per_word, single, word)
        return carry

    lax.fori_loop(0, count, several, 0)

    def drain(s, carry):
        @pl.when(jnp.logical_and(s <= z, z < layers - 1))
        def _():
            wait_bytes(gathered.at[s], z_send.at[0, s])

        @pl.when(jnp.logical_and(s >= z, z > 0))
        def _():
            wait_bytes(gathered.at[s], z_send.at[1, s])

        wait_bytes(packed.at[s, :, pl.ds(1, peers - 1)], a_send.at[s])
        wait_bytes(results.at[s, :, pl.ds(1, peers - 1)], b_send.at[s])

        @pl.when(s != z)
        def _():
            wait_bytes(part.at[s], c_send.at[s])

        return carry

    lax.fori_loop(0, layers, drain, 0)
    for o in range(1, layers):
        meta_copy((z + o) % layers, z).wait_send()
    for o in range(1, cores):
        swap_copy((core + o) % cores, core).wait_send()

    @pl.when(gives_halo)
    def _():
        halo_copy(core).wait_send()

    @pl.when(gives_head)
    def _():
        head_copy(core).wait_send()


def on_device(
    residual,
    pool_input,
    group_maps,
    pool_scale,
    out_proj,
    norm_gain,
    shared_gate,
    shared_up,
    shared_down,
    expert_gate,
    expert_up,
    expert_down,
    expert_ids,
    route_score,
):
    rows, channels = pool_input.shape
    group_width = group_maps.shape[1]
    tokens, top = expert_ids.shape
    width = residual.shape[1]
    size_sp = lax.axis_size("sp")
    cores = lax.axis_size("tp")
    experts = size_sp * cores
    capacity = 3 * tokens * top // (2 * experts)
    cap = -(-capacity // 8) * 8
    layers = layer_count(size_sp)
    peers = experts // layers
    slots = peers * cap
    hidden_width = shared_gate.shape[1]
    expert_width = expert_gate.shape[2]
    cols = min(width, 512)
    blocks = width // cols
    bf16, f32 = jnp.bfloat16, jnp.float32
    dma = pltpu.SemaphoreType.DMA
    routed = (layers, blocks, peers, cap, cols)
    chunks = (layers, blocks, tokens, cols)
    return pl.pallas_call(
        functools.partial(layer_kernel, layers, peers, cores, cap),
        out_shape=pltpu.VMEM((tokens, width), bf16),
        in_specs=[pl.BlockSpec(memory_space=pltpu.HBM)] * 14,
        out_specs=pl.BlockSpec(memory_space=pltpu.VMEM),
        scratch_shapes=[
            pltpu.VMEM((tokens, width), bf16),
            pltpu.VMEM((rows, channels), bf16),
            pltpu.VMEM((cores, halo_rows, channels), bf16),
            pltpu.VMEM((cores, halo_rows, channels), bf16),
            pltpu.VMEM(group_maps.shape, bf16),
            pltpu.VMEM((group_maps.shape[0], 1, group_width), f32),
            pltpu.VMEM((1, width), f32),
            pltpu.VMEM((top, tokens), jnp.int32),
            pltpu.VMEM((top, tokens), f32),
            pltpu.VMEM((cores, rows // cores, channels), bf16),
            pltpu.VMEM((cores, rows // cores, channels), bf16),
            pltpu.VMEM(out_proj.shape, bf16),
            pltpu.VMEM(chunks, bf16),
            pltpu.VMEM((layers, 2 * top, tokens), f32),
            pltpu.VMEM((layers, slots, tokens), bf16),
            pltpu.VMEM((layers, slots, 2 * tokens), bf16),
            pltpu.VMEM(routed, bf16),
            pltpu.VMEM(routed, bf16),
            pltpu.VMEM(routed, bf16),
            pltpu.VMEM(routed, bf16),
            pltpu.VMEM(chunks, bf16),
            pltpu.VMEM((layers + 1, blocks, tokens, cols), bf16),
            pltpu.VMEM((blocks, tokens, cols), f32),
            pltpu.VMEM((layers, slots, expert_width), bf16),
            pltpu.VMEM((width, hidden_width), bf16),
            pltpu.VMEM((width, hidden_width), bf16),
            pltpu.VMEM((hidden_width, width), bf16),
            pltpu.VMEM((width, expert_width), bf16),
            pltpu.VMEM((width, expert_width), bf16),
            pltpu.VMEM((expert_width, width), bf16),
            dma((14,)),
            dma((2,)),
            dma((2, cores)),
            dma((cores,)),
            dma((cores,)),
            dma((2, layers)),
            dma((layers, blocks)),
            dma((layers,)),
            dma((layers,)),
            dma((layers,)),
            dma((layers,)),
            dma((layers,)),
            dma((layers, blocks)),
            dma((layers,)),
            dma((layers + 1, blocks)),
        ],
        compiler_params=pltpu.CompilerParams(
            collective_id=0, has_side_effects=True, vmem_limit_bytes=56 * 1024 * 1024
        ),
    )(
        residual,
        pool_input,
        group_maps,
        pool_scale.reshape(-1, 1, group_width),
        out_proj,
        norm_gain.reshape(1, -1),
        shared_gate,
        shared_up,
        shared_down,
        expert_gate,
        expert_up,
        expert_down,
        expert_ids.T,
        route_score.T,
    )


def solution(mesh):
    in_specs = (
        P(("sp", "tp"), None),
        P("sp", "tp"),
        P(),
        P(),
        P(),
        P(),
        P(),
        P(),
        P(),
        P(("sp", "tp"), None, None),
        P(("sp", "tp"), None, None),
        P(("sp", "tp"), None, None),
        P(("sp", "tp"), None),
        P(("sp", "tp"), None),
    )
    out_specs = P(("sp", "tp"), None)
    return jax.shard_map(
        on_device, mesh=mesh, in_specs=in_specs, out_specs=out_specs, check_vma=False
    )
```

```python
import functools
import math

import jax
import jax.numpy as jnp
from jax import lax
from jax.experimental import pallas as pl
from jax.experimental.pallas import tpu as pltpu
from jax.sharding import PartitionSpec as P

windows = (2, 4, 8, 16)
epsilon = 1e-06
routed_scale = 2.5
halo_rows = 16


def layer_count(size_sp):
    return max(d for d in range(1, math.isqrt(size_sp) + 1) if size_sp % d == 0)


END = (
    " ".join(
        (
            "a00 a01 a02 a03",
            "s a10 a11 a12",
            "a13 a20 a21 a22",
            "a23 e1 b10 a30",
            "a31 a32 e2 b20",
            "a33 c20 c10 b21",
            "e3 b30 b31 b22",
            "b32 c21 b33 b11",
            "c30 b12 e0 c31",
            "c32 b23 c33 b00",
            "c22 b13 c00 b01",
            "b02 b03 c23 c11",
            "c12 c01 c13 c02",
            "c03",
        )
    ),
    " ".join(
        (
            "a00 a01 a02 a03",
            "a10 a11 a12 a13",
            "a20 a21 a22 a23",
            "e0 e1 b10 e2",
            "a30 b20 a31 a32",
            "c10 a33 b21 c20",
            "b00 e3 b30 c21",
            "b31 c30 b32 c31",
            "b33 b11 c32 b22",
            "b23 b12 c11 c33",
            "b01 b13 b02 c22",
            "c23 s c00 c12",
            "b03 c13 c01 c02",
            "c03",
        )
    ),
)
MIDDLE = (
    " ".join(
        (
            "a00 a01 a02 a03",
            "a10 a11 a12 a13",
            "a20 e1 b10 a21",
            "a22 a23 e2 e0",
            "b20 b21 e3 b00",
            "b30 c20 b31 b01",
            "b02 c21 b32 b11",
            "b33 c30 c31 c00",
            "b03 s c32 b22",
            "c01 b23 c10 b12",
            "c33 c02 c03 b13",
            "c22 c23 c11 c12",
            "c13",
        )
    ),
    " ".join(
        (
            "a00 a01 a02 a03",
            "a10 a11 a12 s",
            "a13 e1 e2 b20",
            "a20 a21 a22 a23",
            "b10 e0 b00 b21",
            "e3 b30 c20 b31",
            "b22 b01 b02 c21",
            "b32 b33 c30 b03",
            "c31 c32 c00 c01",
            "c02 b23 c33 b11",
            "b12 c22 c10 c23",
            "c03 b13 c11 c12",
            "c13",
        )
    ),
)


def steps_of(z, core, layers, blocks):
    last = layers - 1
    if (layers, blocks) == (4, 4) and core < len(END):
        steps = []
        for word in (END if z in (0, last) else MIDDLE)[core].split():
            numbers = [int(digit) for digit in word[1:]]
            if word[0] in "ebc" and 2 * z > last:
                numbers[0] = last - numbers[0]
            steps.append((word[0], *numbers))
        return steps
    at = lambda r: sorted({s for s in (z - r, z + r) if 0 <= s < layers})
    reach = max(z, last - z)
    span = range(blocks)
    steps = [("a", 0, k) for k in span] + [("s",)]
    for r in range(1, reach + 2):
        if r <= reach:
            steps += [("a", r, k) for k in span]
        for s in at(r - 1):
            steps += [("e", s)] + [("b", s, k) for k in span]
    for r in range(reach, -1, -1):
        steps += [("c", s, k) for s in at(r) for k in span]
    return steps


def code_of(step, layers, blocks):
    area = layers * blocks
    base = {"a": 0, "b": area, "c": 2 * area, "e": 3 * area, "s": 3 * area + layers}[step[0]]
    if len(step) == 3:
        return base + step[1] * blocks + step[2]
    return base + sum(step[1:])


def layer_kernel(
    layers,
    peers,
    cores,
    cap,
    residual_hbm,
    pool_hbm,
    maps_hbm,
    scale_hbm,
    proj_hbm,
    gain_hbm,
    sg_hbm,
    su_hbm,
    sd_hbm,
    eg_hbm,
    eu_hbm,
    ed_hbm,
    ids_hbm,
    score_hbm,
    out_ref,
    residual,
    pool,
    halo,
    head,
    maps,
    scale,
    gain,
    ids,
    score,
    mixed,
    swapped,
    proj,
    gathered,
    metas,
    tables,
    weigh,
    packed,
    arrived,
    results,
    back,
    part,
    landed,
    acc,
    hidden,
    sg,
    su,
    sd,
    eg,
    eu,
    ed,
    w_sem,
    h_send,
    h_recv,
    x_send,
    x_recv,
    z_send,
    z_recv,
    m_send,
    m_recv,
    a_send,
    a_recv,
    b_send,
    b_recv,
    c_send,
    c_recv,
):
    per_layer = peers // cores
    sp = lax.axis_index("sp")
    size_sp = layers * per_layer
    core = lax.axis_index("tp")
    z = sp // per_layer
    q = sp % per_layer
    me = q * cores + core
    blocks, tokens, cols = acc.shape
    width = blocks * cols
    slots = peers * cap
    top = ids.shape[0]
    rows, channels = pool.shape
    group_width = maps.shape[1]
    groups_here = channels // group_width
    area = layers * blocks
    f32, bf16 = jnp.float32, jnp.bfloat16

    def in_column(s):
        return (s * per_layer + q, core)

    def in_layer(p):
        return (z * per_layer + p // cores, p % cores)

    def remote(src, dst, send, recv, to):
        return pltpu.make_async_remote_copy(
            src_ref=src,
            dst_ref=dst,
            send_sem=send,
            recv_sem=recv,
            device_id=to,
            device_id_type=pl.DeviceIdType.MESH,
        )

    def tell(to):
        pl.semaphore_signal(
            pltpu.get_barrier_semaphore(), inc=1, device_id=to,
            device_id_type=pl.DeviceIdType.MESH,
        )

    pairs = (
        (pool_hbm, pool),
        (ids_hbm, ids),
        (score_hbm, score),
        (maps_hbm, maps),
        (scale_hbm, scale),
        (proj_hbm, proj),
        (residual_hbm, residual),
        (gain_hbm, gain),
        (sg_hbm, sg),
        (su_hbm, su),
        (sd_hbm, sd),
        (eg_hbm.at[0], eg),
        (eu_hbm.at[0], eu),
        (ed_hbm.at[0], ed),
    )
    loads = [pltpu.make_async_copy(a, b, w_sem.at[i]) for i, (a, b) in enumerate(pairs)]
    for load in loads[:5]:
        load.start()
    for o in range(1, layers):
        tell(in_column((z + o) % layers))
    for o in range(1, peers):
        tell(in_layer((me + o) % peers))

    takes_halo = jnp.logical_and(sp > 0, core == 0)
    gives_halo = sp < size_sp - 1

    @pl.when(takes_halo)
    def _():
        for c in range(cores):
            tell((sp - 1, c))

    for load in loads[5:8]:
        load.start()

    half = rows // cores

    def mix(before, own, start, c):
        place = start + lax.broadcasted_iota(jnp.int32, (own.shape[0], group_width), 0)
        out = []
        for g in range(groups_here):
            lanes = slice(g * group_width, (g + 1) * group_width)
            here = own[:, lanes]
            total = jnp.concatenate([before[:, lanes], here], axis=0)
            span = 1
            while span < windows[g % 4]:
                total = total + pltpu.roll(total, span, 0)
                span = span * 2
            divisor = jnp.minimum(place + 1, span).astype(f32)
            contrast = (total[halo_rows:] / divisor - here).astype(bf16)
            group = c * groups_here + g
            mapped = jnp.dot(contrast, maps[group], preferred_element_type=f32)
            out.append((mapped * scale[group]).astype(bf16))
        return jnp.concatenate(out, axis=1)

    for i in (0, 3, 4):
        loads[i].wait()
    for c in range(cores):
        start = c * half
        before = pool[max(start - halo_rows, 0) : max(start, halo_rows)].astype(f32)
        if c == 0:
            before = jnp.zeros_like(before)
        mixed[c] = mix(before, pool[start : start + half].astype(f32), sp * rows + start, core)

    pl.semaphore_wait(
        pltpu.get_barrier_semaphore(),
        layers - 1 + peers - 1 + jnp.where(gives_halo, 1, 0),
    )

    def halo_copy(source):
        return remote(
            pool.at[pl.ds(rows - halo_rows, halo_rows)], halo.at[source], h_send.at[0],
            h_recv.at[0, source], (jnp.minimum(sp + 1, size_sp - 1), 0),
        )

    def head_copy(source):
        return remote(
            pool.at[pl.ds(0, halo_rows)], head.at[source], h_send.at[1],
            h_recv.at[1, source], (sp, 0),
        )

    def swap_copy(p, source):
        return remote(
            mixed.at[p], swapped.at[source], x_send.at[p], x_recv.at[source], (sp, p)
        )

    @pl.when(gives_halo)
    def _():
        halo_copy(core).start()

    for o in range(1, cores):
        swap_copy((core + o) % cores, core).start()

    gives_head = jnp.logical_and(sp > 0, core > 0)

    @pl.when(gives_head)
    def _():
        head_copy(core).start()

    def meta_copy(target, source):
        return remote(
            metas.at[source], metas.at[source], m_send.at[target], m_recv.at[source],
            in_column(target),
        )

    for load in loads[8:11]:
        load.start()

    def neighbour(side):
        return in_column(jnp.clip(jnp.where(side == 0, z + 1, z - 1), 0, layers - 1))

    def chunk_copy(s, k, side):
        return remote(
            gathered.at[s, k], gathered.at[s, k], z_send.at[side, s], z_recv.at[s, k],
            neighbour(side),
        )

    def pack_copy(s, k, p, source):
        return remote(
            packed.at[s, k, p], arrived.at[s, k, source], a_send.at[s],
            a_recv.at[s], in_layer(p),
        )

    def back_copy(s, k, p, source):
        return remote(
            results.at[s, k, p], back.at[s, k, source], b_send.at[s],
            b_recv.at[s, k], in_layer(p),
        )

    def own_pack(s, k):
        return pltpu.make_async_copy(
            packed.at[s, k, me], arrived.at[s, k, me], a_recv.at[s]
        )

    def own_back(s, k):
        return pltpu.make_async_copy(
            results.at[s, k, me], back.at[s, k, me], b_recv.at[s, k]
        )

    def part_copy(s, k, side):
        slot = jnp.where(jnp.logical_and(side == 1, s == z - 1), layers, s)
        return remote(
            part.at[s, k], landed.at[slot, k], c_send.at[s], c_recv.at[slot, k],
            neighbour(side),
        )

    def wait_bytes(ref, sem):
        pltpu.make_async_copy(ref, ref, sem).wait()

    far_first = sorted(range(1, peers), key=lambda o: (o % cores, -o % 3, o))

    for load in loads[11:]:
        load.start()
    loads[1].wait()
    loads[2].wait()
    experts = layers * peers
    ids_now = ids[...]
    score_now = score[...]
    expert_at = lax.broadcasted_iota(jnp.int32, (experts, tokens), 0)
    named = [(ids_now[k : k + 1] == expert_at).astype(f32) for k in range(top)]
    named_any = functools.reduce(jnp.add, named).astype(bf16)
    earlier = (
        lax.broadcasted_iota(jnp.int32, (tokens, tokens), 0)
        < lax.broadcasted_iota(jnp.int32, (tokens, tokens), 1)
    ).astype(bf16)
    rank = jnp.dot(named_any, earlier, preferred_element_type=f32)
    shares = score_now / jnp.sum(score_now, axis=0, keepdims=True) * routed_scale
    slot = [
        ids_now[k : k + 1].astype(f32) * cap + jnp.sum(rank * named[k], axis=0, keepdims=True)
        for k in range(top)
    ]
    metas[z] = jnp.concatenate(slot + [shares], axis=0)

    for o in range(1, layers):
        meta_copy((z + o) % layers, z).start()

    for load in loads[5:8]:
        load.wait()

    def channels_of(c):
        return pl.ds(pl.multiple_of(c * channels, channels), channels)

    def project_own():
        for k in range(blocks):
            lanes = slice(k * cols, (k + 1) * cols)
            acc[k] = residual[:, lanes].astype(f32) + jnp.dot(
                mixed[core], proj[channels_of(core), lanes], preferred_element_type=f32
            )

    @pl.when(jnp.logical_not(takes_halo))
    def _():
        project_own()

    for o in range(1, cores):
        p = (core + o) % cores
        swap_copy(p, p).wait_recv()

    @pl.when(takes_halo)
    def _():
        for c in range(cores):
            halo_copy(c).wait_recv()
            own = pool[:halo_rows]
            if c > 0:
                head_copy(c).wait_recv()
                own = head[c]
            fixed = mix(halo[c].astype(f32), own.astype(f32), sp * rows, c)
            if c == 0:
                mixed[0, :halo_rows] = fixed
            else:
                swapped[c, :halo_rows] = fixed

    @pl.when(takes_halo)
    def _():
        project_own()

    for k in range(blocks):
        lanes = slice(k * cols, (k + 1) * cols)
        total = acc[k]
        for o in range(1, cores):
            p = (core + o) % cores
            total = total + jnp.dot(
                swapped[p], proj[channels_of(p), lanes], preferred_element_type=f32
            )
        acc[k] = total
    squares = jnp.zeros((tokens, 1), f32)
    for k in range(blocks):
        settled = acc[k].astype(bf16).astype(f32)
        acc[k] = settled
        squares = squares + jnp.sum(settled * settled, axis=1, keepdims=True)
    inverse = lax.rsqrt(squares / width + epsilon)
    for k in range(blocks):
        gathered[z, k] = (acc[k] * inverse * gain[:, k * cols : (k + 1) * cols]).astype(bf16)

        @pl.when(z < layers - 1)
        def _():
            chunk_copy(z, k, 0).start()

        @pl.when(z > 0)
        def _():
            chunk_copy(z, k, 1).start()

    def prepare(s):
        rows_now = metas[s]
        ids_down = lax.broadcasted_iota(jnp.int32, (slots, tokens), 0).astype(f32)
        ids_down = ids_down + (z * slots).astype(f32)
        table = jnp.zeros((slots, tokens), f32)
        value = jnp.zeros((slots, tokens), f32)
        for k in range(top):
            hit = ids_down == rows_now[k : k + 1]
            table = jnp.where(hit, 1.0, table)
            value = jnp.where(hit, rows_now[top + k : top + k + 1], value)
        tables[s] = table.astype(bf16)
        high = value.astype(bf16)
        weigh[s, :, :tokens] = high
        weigh[s, :, tokens:] = (value - high.astype(f32)).astype(bf16)

    def arrive(r, k):
        def one(side, carry):
            s = jnp.where(side == 0, z - r, z + r)
            here = jnp.logical_and(s >= 0, s < layers)
            here = jnp.logical_and(here, jnp.logical_or(r > 0, side == 0))
            far = jnp.logical_and(here, r > 0)
            onward = jnp.logical_and(far, jnp.where(side == 0, z < layers - 1, z > 0))
            s = jnp.clip(s, 0, layers - 1)

            @pl.when(far)
            def _():
                chunk_copy(s, k, 0).wait_recv()

            @pl.when(onward)
            def _():
                chunk_copy(s, k, side).start()

            @pl.when(jnp.logical_and(far, k == 0))
            def _():
                meta_copy(z, s).wait_recv()

            @pl.when(jnp.logical_and(here, k == 0))
            def _():
                prepare(s)

            @pl.when(here)
            def _():
                got = jnp.dot(tables[s], gathered[s, k], preferred_element_type=f32)
                packed[s, k] = got.astype(bf16).reshape(peers, cap, cols)
                for o in far_first:
                    pack_copy(s, k, (me + o) % peers, me).start()
                own_pack(s, k).start()

            return carry

        lax.fori_loop(0, 2, one, 0)

    def mlp(tall, w_gate, w_up):
        gate = jnp.dot(tall, w_gate[...], preferred_element_type=f32)
        up = jnp.dot(tall, w_up[...], preferred_element_type=f32)
        return (gate / (1.0 + jnp.exp(-gate)) * up).astype(bf16)

    def expert(s):
        wait_bytes(arrived.at[s], a_recv.at[s])
        tall = jnp.concatenate(
            [arrived[s, k].reshape(slots, cols) for k in range(blocks)], axis=1
        )
        hidden[s] = mlp(tall, eg, eu)

    def give_back(s, k):
        lanes = pl.ds(pl.multiple_of(k * cols, cols), cols)
        got = jnp.dot(hidden[s], ed[:, lanes], preferred_element_type=f32)
        results[s, k] = got.astype(bf16).reshape(peers, cap, cols)
        for o in far_first:
            back_copy(s, k, (me + o) % peers, me).start()
        own_back(s, k).start()

    def combine(s, k):
        below = jnp.logical_and(s >= z, z > 0)
        above = jnp.logical_and(s <= z, z < layers - 1)
        over = jnp.where(s == z, layers, s)
        wait_bytes(back.at[s, k], b_recv.at[s, k])
        both = lax.dot_general(
            weigh[s], back[s, k].reshape(slots, cols), (((0,), (0,)), ((), ())),
            preferred_element_type=f32,
        )
        got = both[:tokens] + both[tokens:]

        @pl.when(below)
        def _():
            wait_bytes(landed.at[s, k], c_recv.at[s, k])

        @pl.when(above)
        def _():
            wait_bytes(landed.at[over, k], c_recv.at[over, k])

        got = got + jnp.where(below, landed[s, k].astype(f32), 0.0)
        got = got + jnp.where(above, landed[over, k].astype(f32), 0.0)

        @pl.when(s == z)
        def _():
            lanes = pl.ds(pl.multiple_of(k * cols, cols), cols)
            out_ref[:, lanes] = (acc[k] + got).astype(bf16)

        @pl.when(s != z)
        def _():
            part[s, k] = got.astype(bf16)
            part_copy(s, k, jnp.where(s > z, 0, 1)).start()

    def shared():
        for load in loads[8:11]:
            load.wait()
        tall = jnp.concatenate([gathered[z, k] for k in range(blocks)], axis=1)
        inner = mlp(tall, sg, su)
        for k in range(blocks):
            acc[k] = acc[k] + jnp.dot(
                inner, sd[:, k * cols : (k + 1) * cols], preferred_element_type=f32
            )

    plans = {
        (s, c): [code_of(step, layers, blocks) for step in steps_of(s, c, layers, blocks)]
        for s in range(layers)
        for c in range(cores)
    }
    nothing = 3 * area + layers + 1
    base = 1 << nothing.bit_length()
    per_word = 30 // nothing.bit_length()
    count = -(-max(len(plan) for plan in plans.values()) // per_word)
    words = []
    for i in range(count):
        word = jnp.int32(0)
        for (s, c), plan in plans.items():
            codes = plan[i * per_word : (i + 1) * per_word]
            codes = codes + [nothing] * (per_word - len(codes))
            packed_codes = sum(code * base**j for j, code in enumerate(codes))
            word = jnp.where(jnp.logical_and(z == s, core == c), packed_codes, word)
        words.append(word)

    def act(code):
        number = code % area
        s = number // blocks
        k = number % blocks

        @pl.when(code < area)
        def _():
            arrive(s, k)

        @pl.when(code == 2 * blocks - 1)
        def _():
            for load in loads[11:]:
                load.wait()

        @pl.when(jnp.logical_and(code >= area, code < 2 * area))
        def _():
            give_back(s, k)

        @pl.when(jnp.logical_and(code >= 2 * area, code < 3 * area))
        def _():
            combine(s, k)

        @pl.when(jnp.logical_and(code >= 3 * area, code < 3 * area + layers))
        def _():
            expert(code - 3 * area)

        @pl.when(code == 3 * area + layers)
        def _():
            shared()

    def several(i, carry):
        word = words[0]
        for j in range(1, count):
            word = jnp.where(i == j, words[j], word)

        def single(j, word):
            act(word % base)
            return word // base

        lax.fori_loop(0, per_word, single, word)
        return carry

    lax.fori_loop(0, count, several, 0)

    def drain(s, carry):
        @pl.when(jnp.logical_and(s <= z, z < layers - 1))
        def _():
            wait_bytes(gathered.at[s], z_send.at[0, s])

        @pl.when(jnp.logical_and(s >= z, z > 0))
        def _():
            wait_bytes(gathered.at[s], z_send.at[1, s])

        wait_bytes(packed.at[s, :, pl.ds(1, peers - 1)], a_send.at[s])
        wait_bytes(results.at[s, :, pl.ds(1, peers - 1)], b_send.at[s])

        @pl.when(s != z)
        def _():
            wait_bytes(part.at[s], c_send.at[s])

        return carry

    lax.fori_loop(0, layers, drain, 0)
    for o in range(1, layers):
        meta_copy((z + o) % layers, z).wait_send()
    for o in range(1, cores):
        swap_copy((core + o) % cores, core).wait_send()

    @pl.when(gives_halo)
    def _():
        halo_copy(core).wait_send()

    @pl.when(gives_head)
    def _():
        head_copy(core).wait_send()


def on_device(
    residual,
    pool_input,
    group_maps,
    pool_scale,
    out_proj,
    norm_gain,
    shared_gate,
    shared_up,
    shared_down,
    expert_gate,
    expert_up,
    expert_down,
    expert_ids,
    route_score,
):
    rows, channels = pool_input.shape
    group_width = group_maps.shape[1]
    tokens, top = expert_ids.shape
    width = residual.shape[1]
    size_sp = lax.axis_size("sp")
    cores = lax.axis_size("tp")
    experts = size_sp * cores
    capacity = 3 * tokens * top // (2 * experts)
    cap = -(-capacity // 8) * 8
    layers = layer_count(size_sp)
    peers = experts // layers
    slots = peers * cap
    hidden_width = shared_gate.shape[1]
    expert_width = expert_gate.shape[2]
    cols = min(width, 512)
    blocks = width // cols
    bf16, f32 = jnp.bfloat16, jnp.float32
    dma = pltpu.SemaphoreType.DMA
    routed = (layers, blocks, peers, cap, cols)
    chunks = (layers, blocks, tokens, cols)
    return pl.pallas_call(
        functools.partial(layer_kernel, layers, peers, cores, cap),
        out_shape=pltpu.VMEM((tokens, width), bf16),
        in_specs=[pl.BlockSpec(memory_space=pltpu.HBM)] * 14,
        out_specs=pl.BlockSpec(memory_space=pltpu.VMEM),
        scratch_shapes=[
            pltpu.VMEM((tokens, width), bf16),
            pltpu.VMEM((rows, channels), bf16),
            pltpu.VMEM((cores, halo_rows, channels), bf16),
            pltpu.VMEM((cores, halo_rows, channels), bf16),
            pltpu.VMEM(group_maps.shape, bf16),
            pltpu.VMEM((group_maps.shape[0], 1, group_width), f32),
            pltpu.VMEM((1, width), f32),
            pltpu.VMEM((top, tokens), jnp.int32),
            pltpu.VMEM((top, tokens), f32),
            pltpu.VMEM((cores, rows // cores, channels), bf16),
            pltpu.VMEM((cores, rows // cores, channels), bf16),
            pltpu.VMEM(out_proj.shape, bf16),
            pltpu.VMEM(chunks, bf16),
            pltpu.VMEM((layers, 2 * top, tokens), f32),
            pltpu.VMEM((layers, slots, tokens), bf16),
            pltpu.VMEM((layers, slots, 2 * tokens), bf16),
            pltpu.VMEM(routed, bf16),
            pltpu.VMEM(routed, bf16),
            pltpu.VMEM(routed, bf16),
            pltpu.VMEM(routed, bf16),
            pltpu.VMEM(chunks, bf16),
            pltpu.VMEM((layers + 1, blocks, tokens, cols), bf16),
            pltpu.VMEM((blocks, tokens, cols), f32),
            pltpu.VMEM((layers, slots, expert_width), bf16),
            pltpu.VMEM((width, hidden_width), bf16),
            pltpu.VMEM((width, hidden_width), bf16),
            pltpu.VMEM((hidden_width, width), bf16),
            pltpu.VMEM((width, expert_width), bf16),
            pltpu.VMEM((width, expert_width), bf16),
            pltpu.VMEM((expert_width, width), bf16),
            dma((14,)),
            dma((2,)),
            dma((2, cores)),
            dma((cores,)),
            dma((cores,)),
            dma((2, layers)),
            dma((layers, blocks)),
            dma((layers,)),
            dma((layers,)),
            dma((layers,)),
            dma((layers,)),
            dma((layers,)),
            dma((layers, blocks)),
            dma((layers,)),
            dma((layers + 1, blocks)),
        ],
        compiler_params=pltpu.CompilerParams(
            collective_id=0, has_side_effects=True, vmem_limit_bytes=56 * 1024 * 1024
        ),
    )(
        residual,
        pool_input,
        group_maps,
        pool_scale.reshape(-1, 1, group_width),
        out_proj,
        norm_gain.reshape(1, -1),
        shared_gate,
        shared_up,
        shared_down,
        expert_gate,
        expert_up,
        expert_down,
        expert_ids.T,
        route_score.T,
    )


def solution(mesh):
    in_specs = (
        P(("sp", "tp"), None),
        P("sp", "tp"),
        P(),
        P(),
        P(),
        P(),
        P(),
        P(),
        P(),
        P(("sp", "tp"), None, None),
        P(("sp", "tp"), None, None),
        P(("sp", "tp"), None, None),
        P(("sp", "tp"), None),
        P(("sp", "tp"), None),
    )
    out_specs = P(("sp", "tp"), None)
    return jax.shard_map(
        on_device, mesh=mesh, in_specs=in_specs, out_specs=out_specs, check_vma=False
    )
```
